128 devices in a mesh: sp: 64 (over z, y, x), tp: 2 (over core).
Axes of the slice: x: 4, y: 4, z: 4, core: 2. Of those that a mesh axis runs over, the one named last changes fastest.
Arguments:
- stream: bfloat16 [16384, 2048], P(('sp', 'tp')), may hold values from -3 to 3
- query_narrow: bfloat16 [16384, 1024], P('sp', 'tp'), may hold values from -6 to 6
- key_narrow: bfloat16 [16384, 128], P('sp', 'tp'), may hold values from -6 to 6
- value_narrow: bfloat16 [16384, 128], P('sp', 'tp'), may hold values from -6 to 6
- query_broad: bfloat16 [16384, 1024], P('sp', 'tp'), may hold values from -6 to 6
- key_broad: bfloat16 [16384, 256], P('sp', 'tp'), may hold values from -6 to 6
- value_broad: bfloat16 [16384, 256], P('sp', 'tp'), may hold values from -6 to 6
- narrow_query_gain: float32 [64], replicated, may hold values from 1.5 to 9
- narrow_key_gain: float32 [64], replicated, may hold values from 1.5 to 9
- broad_query_gain: float32 [128], replicated, may hold values from 1.5 to 9
- broad_key_gain: float32 [128], replicated, may hold values from 1.5 to 9
- out_weight: bfloat16 [2048, 2048], replicated, may hold values from -0.125 to 0.125
- norm_gain: float32 [2048], replicated, may hold values from 0.1 to 1.9
- gate_weight: bfloat16 [64, 2048, 1024], P('sp', None, 'tp'), may hold values from -0.125 to 0.125
- up_weight: bfloat16 [64, 2048, 1024], P('sp', None, 'tp'), may hold values from -0.125 to 0.125
- down_weight: bfloat16 [64, 1024, 2048], P('sp', 'tp'), may hold values from -0.1875 to 0.1875
- route_ids: int32 [16384, 2], P(('sp', 'tp')), may hold values from 0 to 63, all different within a row; in each aligned block of 128 rows (0 to 127, 128 to 255, ...) at most 8 rows name the same one
- route_weights: float32 [16384, 2], P(('sp', 'tp')), may hold values from 0.1 to 1
Outputs:
- result: bfloat16 [16384, 2048], P(('sp', 'tp'))
The draws below stay inside these ranges and needn't reach their ends.
Inputs may be any that keep to these rules, and one draw needn't show every extreme that they name: `route_ids`: in each aligned block of 128 rows no expert is named by more than 8 rows, a bound that some block reaches.
All inputs are finite; a program needn't handle non-finite values.
Results may differ from the reference program's by a relative error of at most 0.015.
The reference program's roundings to bfloat16 on the way count: a program that leaves them out, or rounds other values in their place, can miss the bound.
Values may be sent and summed in bfloat16 or wider, within the bound.
A program may use at most 128 MiB of HBM per device.

```python
import math
import jax
import jax.numpy as jnp
import numpy as np
from jax import lax

D = 2048
HA = 16
KA = 2
DA = 64
HB = 8
KB = 2
DB = 128
FE = 1024
TOPK = 2
GRID_W = 128
TOKENS = 16384
ROWS_DEV = 128
EXPERTS = 64
MIX = 2048
CAP = 8
N_SP = 64
N_TP = 2


def plain_rows(key, salt, width):
    return jnp.clip(jax.random.normal(jax.random.fold_in(key, salt), (TOKENS, width), jnp.float32), -6.0, 6.0)


def aligned_queries(key, salt_query, salt_key, heads, heads_kv, dim):
    queries = plain_rows(key, salt_query, heads * dim)
    return queries.astype(jnp.bfloat16)


def spread_gain(key, salt, width):
    sample = jax.random.uniform(jax.random.fold_in(key, salt), (width,), jnp.float32)
    return 1.5 + 0.5 * sample


def draw_key_narrow(key, part):
    return plain_rows(key, 101, KA * DA).astype(jnp.bfloat16)


def draw_query_narrow(key, part):
    return aligned_queries(key, 201, 101, HA, KA, DA)


def draw_key_broad(key, part):
    return plain_rows(key, 102, KB * DB).astype(jnp.bfloat16)


def draw_query_broad(key, part):
    return aligned_queries(key, 202, 102, HB, KB, DB)


def draw_narrow_query_gain(key, part):
    return spread_gain(key, 301, DA)


def draw_narrow_key_gain(key, part):
    return spread_gain(key, 302, DA)


def draw_broad_query_gain(key, part):
    return spread_gain(key, 303, DB)


def draw_broad_key_gain(key, part):
    return spread_gain(key, 304, DB)


def level_of(stream_key, shape, shards, least, top_value):
    loudness, own = 1.0, jax.random.fold_in(stream_key, 6)
    for position, shards_of in shards:
        heights = jnp.exp(jax.random.uniform(jax.random.fold_in(own, position), (shards_of,), jnp.float32, least / len(shards), top_value / len(shards)))
        loudness = loudness * jnp.repeat(heights, shape[position] // shards_of).reshape([-1 if axis == position else 1 for axis in range(len(shape))])
    return loudness


def shared_out(rng, own, number, rows, number_of, top, most, lean):
    ranking = jax.random.permutation(rng, number_of)
    packed, common = load_shares(number_of, rows * top, most, lean, True), load_shares(number_of, rows * top, most, lean, False)
    places = jnp.arange(number_of)

    def named(sizes, turn):
        used = int((sizes > 0).sum())
        fixed = max(1, used // 4)
        moved = fixed + (places - fixed + turn * (used - fixed)) % max(1, number_of - fixed)
        return jnp.zeros((number_of,), jnp.int32).at[ranking[jnp.where(places < fixed, places, moved)]].set(jnp.asarray(sizes, jnp.int32))

    sizes = jnp.where(number % 4 == 0, named(packed, number // 4), named(common, number - number // 4 - 1))
    mixed = jax.random.permutation(jax.random.fold_in(own, 3), number_of)
    donor, taker = mixed[0:number_of // 2 * 2:2], mixed[1:number_of // 2 * 2:2]
    margin = jnp.minimum(sizes[donor] - 1, most - sizes[taker]) // 2
    margin = jnp.where((donor == ranking[0]) | (taker == ranking[0]) | (sizes[taker] == 0), 0, jnp.maximum(margin, 0))
    moved = jax.random.randint(jax.random.fold_in(own, 4), (number_of // 2,), 0, 1 << 20) % (margin + 1)
    sizes = sizes.at[donor].add(-moved).at[taker].add(moved)
    items = jnp.searchsorted(jnp.cumsum(sizes), jnp.arange(rows * top), side="right").astype(jnp.int32)
    grid = items.reshape(top, rows).T
    grid = grid[jax.random.permutation(jax.random.fold_in(own, 1), rows)]
    turn = jax.random.randint(jax.random.fold_in(own, 2), (rows, 1), 0, top)
    return jnp.take_along_axis(grid, (jnp.arange(top)[None, :] + turn) % top, axis=1)


def load_shares(number_of, total, reach, lean, full):
    weights = [(1 << 20) // math.isqrt(standing ** lean) + 1 for standing in range(1, number_of + 1)]
    largest = reach if full else min(reach, max(-(-total // number_of), total * weights[0] // sum(weights)))
    least = 1 if total - largest >= number_of - 1 else 0
    given, surplus = [largest] + [least] * (number_of - 1), total - largest - least * (number_of - 1)
    while surplus > 0:
        free = [i for i in range(1, number_of) if given[i] < largest] or [i for i in range(1, number_of) if given[i] < reach]
        mass, remaining = sum([weights[i] for i in free]), surplus
        for i in free:
            extra = min(reach - given[i], max(1, remaining * weights[i] // mass), surplus)
            given[i] = given[i] + extra
            surplus = surplus - extra
    return np.array(given)


def noise(stream_key, shape, scale, reach, cuts=(), held_as=jnp.bfloat16):
    array = jax.random.normal(stream_key, shape, jnp.float32) * scale
    if len(cuts) > 0:
        array = level_of(stream_key, shape, cuts, -0.22, 0.18) * array
    return jnp.clip(array, min=-reach, max=reach).astype(held_as)


def setup_inputs(seed: int = 0) -> dict:
    streams_of = jax.random.split(jax.random.key(seed), 19)
    stream = noise(streams_of[0], (TOKENS, D), 0.5, 3.0, ((0, 128),))
    query_narrow = draw_query_narrow(jax.random.fold_in(streams_of[18], 71), 0)
    key_narrow = draw_key_narrow(jax.random.fold_in(streams_of[18], 71), 0)
    value_narrow = noise(streams_of[3], (TOKENS, KA * DA), 1.0, 6.0, ((0, 64), (1, 2)))
    query_broad = draw_query_broad(jax.random.fold_in(streams_of[18], 71), 0)
    key_broad = draw_key_broad(jax.random.fold_in(streams_of[18], 71), 0)
    value_broad = noise(streams_of[6], (TOKENS, KB * DB), 1.0, 6.0, ((0, 64), (1, 2)))
    narrow_query_gain = draw_narrow_query_gain(jax.random.fold_in(streams_of[18], 71), 0)
    narrow_key_gain = draw_narrow_key_gain(jax.random.fold_in(streams_of[18], 71), 0)
    broad_query_gain = draw_broad_query_gain(jax.random.fold_in(streams_of[18], 71), 0)
    broad_key_gain = draw_broad_key_gain(jax.random.fold_in(streams_of[18], 71), 0)
    out_weight = noise(streams_of[11], (MIX, D), MIX ** -0.5, 0.125)
    norm_gain = jnp.clip(1.0 + 0.18 * jax.random.normal(streams_of[12], (D,), jnp.float32), 0.1, 1.9)
    gate_weight = noise(streams_of[13], (EXPERTS, D, FE), D ** -0.5, 0.125, ((0, 64), (2, 2)))
    up_weight = noise(streams_of[14], (EXPERTS, D, FE), D ** -0.5, 0.125, ((0, 64), (2, 2)))
    down_weight = noise(streams_of[15], (EXPERTS, FE, D), FE ** -0.5, 0.1875, ((0, 64), (1, 2)))
    route_ids_keys = jax.random.split(jax.random.fold_in(streams_of[16], 1), TOKENS // ROWS_DEV)
    route_ids_turns = jax.random.permutation(jax.random.fold_in(streams_of[16], 3), TOKENS // ROWS_DEV)
    route_ids = jax.vmap(lambda own, number: shared_out(jax.random.fold_in(streams_of[16], 2), own, number, ROWS_DEV, EXPERTS, TOPK, CAP, 1))(route_ids_keys, route_ids_turns).reshape((TOKENS, TOPK))
    route_weights = jnp.clip(0.1 + 0.9 * jax.random.uniform(streams_of[17], (TOKENS, TOPK), jnp.float32) ** level_of(streams_of[17], (TOKENS, TOPK), ((0, 128),), -0.2, 0.2), 0.1, 1.0)
    return {"stream": stream, "query_narrow": query_narrow, "key_narrow": key_narrow, "value_narrow": value_narrow, "query_broad": query_broad, "key_broad": key_broad, "value_broad": value_broad, "narrow_query_gain": narrow_query_gain, "narrow_key_gain": narrow_key_gain, "broad_query_gain": broad_query_gain, "broad_key_gain": broad_key_gain, "out_weight": out_weight, "norm_gain": norm_gain, "gate_weight": gate_weight, "up_weight": up_weight, "down_weight": down_weight, "route_ids": route_ids, "route_weights": route_weights}


eps = 1e-06
theta = 10000.0
query_block = 128

def rotate_grid(normed, positions):
    count, heads, dim = normed.shape
    freqs = dim // 4
    inverse = theta ** (-jnp.arange(freqs, dtype=jnp.float32) / freqs)
    rows = (positions // GRID_W).astype(jnp.float32)
    cols = (positions % GRID_W).astype(jnp.float32)
    angles = jnp.stack([rows[:, None] * inverse, cols[:, None] * inverse], axis=1)
    cosine = jnp.cos(angles)[:, None]
    sine = jnp.sin(angles)[:, None]
    split = normed.reshape(count, heads, 2, 2, freqs)
    first = split[..., 0, :]
    second = split[..., 1, :]
    turned = jnp.stack([first * cosine - second * sine, second * cosine + first * sine], axis=-2)
    return turned.reshape(count, heads, dim)

def prepare(raw, gain, dim, positions):
    count = raw.shape[0]
    values = raw.astype(jnp.float32).reshape(count, -1, dim)
    scaled = values * lax.rsqrt(lax.optimization_barrier(jnp.mean(values * values, axis=-1, keepdims=True)) + eps) * gain
    return rotate_grid(scaled, positions).reshape(count, -1).astype(jnp.bfloat16)

def attend(queries, keys, values, heads, heads_kv, dim):
    groups = heads // heads_kv
    blocks = lax.optimization_barrier(queries).astype(jnp.float32).reshape(TOKENS // query_block, query_block, heads_kv, groups, dim)
    keys3 = lax.optimization_barrier(keys).astype(jnp.float32).reshape(TOKENS, heads_kv, dim)
    values3 = values.astype(jnp.float32).reshape(TOKENS, heads_kv, dim)

    def one(block):
        scores = jnp.einsum('qhgd,khd->hgqk', block, keys3) * dim ** (-0.5)
        top = lax.optimization_barrier(jnp.max(scores, axis=-1, keepdims=True))
        weights = jnp.exp(scores - top)
        sums = lax.optimization_barrier(jnp.sum(weights, axis=-1))
        rounded = lax.optimization_barrier(weights.astype(jnp.bfloat16)).astype(jnp.float32)
        summed = jnp.einsum('hgqk,khd->qhgd', rounded, values3)
        return (summed / jnp.transpose(sums, (2, 0, 1))[..., None]).astype(jnp.bfloat16)
    out = lax.map(one, blocks)
    return out.reshape(TOKENS, heads * dim)

def expert_out(rows, gate_w, up_w, down_w):
    gate = jnp.dot(rows, gate_w, preferred_element_type=jnp.float32)
    upper = jnp.dot(rows, up_w, preferred_element_type=jnp.float32)
    hidden = (jax.nn.silu(gate) * upper).astype(jnp.bfloat16)
    width = hidden.shape[1] // N_TP
    total = jnp.zeros((rows.shape[0], down_w.shape[1]), jnp.float32)
    for block_index in range(N_TP):
        lower = block_index * width
        piece = jnp.dot(hidden[:, lower:lower + width], down_w[lower:lower + width], preferred_element_type=jnp.float32).astype(jnp.bfloat16)
        total = total + lax.optimization_barrier(piece).astype(jnp.float32)
    return total.astype(jnp.bfloat16)

def reference(stream, query_narrow, key_narrow, value_narrow, query_broad, key_broad, value_broad, narrow_query_gain, narrow_key_gain, broad_query_gain, broad_key_gain, out_weight, norm_gain, gate_weight, up_weight, down_weight, route_ids, route_weights):
    positions = jnp.arange(TOKENS, dtype=jnp.int32)
    queries_n = prepare(query_narrow, narrow_query_gain, DA, positions)
    keys_n = prepare(key_narrow, narrow_key_gain, DA, positions)
    queries_b = prepare(query_broad, broad_query_gain, DB, positions)
    keys_b = prepare(key_broad, broad_key_gain, DB, positions)
    heads_n = attend(queries_n, keys_n, value_narrow, HA, KA, DA)
    heads_b = attend(queries_b, keys_b, value_broad, HB, KB, DB)
    heads = jnp.concatenate([heads_n, heads_b], axis=1)
    mixed = jnp.dot(heads, out_weight, preferred_element_type=jnp.float32)
    mixed_stream = (stream.astype(jnp.float32) + mixed).astype(jnp.bfloat16)
    wide = mixed_stream.astype(jnp.float32)
    normed = (wide * lax.rsqrt(lax.optimization_barrier(jnp.mean(wide * wide, axis=-1, keepdims=True)) + eps) * norm_gain).astype(jnp.bfloat16)
    limit = CAP * N_SP * N_TP

    def step(total, expert):
        number, gate_w, up_w, down_w = expert
        chosen = route_ids == number
        weight = lax.optimization_barrier(jnp.sum(jnp.where(chosen, route_weights, 0.0), axis=1))
        marked = jnp.where(jnp.any(chosen, axis=1), 0, 1).astype(jnp.int32)
        order = jnp.argsort(marked, stable=True)[:limit].astype(jnp.int32)
        out = expert_out(normed[order], gate_w, up_w, down_w)
        total = total.at[order].add(weight[order][:, None] * out.astype(jnp.float32))
        return (total, None)
    total, _ = lax.scan(step, jnp.zeros((TOKENS, D), jnp.float32), (jnp.arange(EXPERTS, dtype=jnp.int32), gate_weight, up_weight, down_weight))
    return (wide + total).astype(jnp.bfloat16)
```

```python
import functools
import math

import jax
import jax.numpy as jnp
import numpy as np
from jax import lax
from jax.experimental import pallas as pl
from jax.experimental.pallas import tpu as pltpu
from jax.sharding import PartitionSpec as P

F32 = jnp.float32
BF = jnp.bfloat16
MESH = pl.DeviceIdType.MESH
eps = 1e-06
theta = 10000.0
LOG2E = math.log2(math.e)
NB = 4
ORDERS = ((2, 1, 0), (1, 0, 2), (0, 2, 1))
OFFSETS = (0, -1, 1, 2)


def sem_index(piece, phase, item, way):
    base = (0, 4, 20)[phase]
    return piece * 36 + base + item * 4 + way


def inverse_table():
    parts = []
    for dim in (64, 128):
        freqs = dim // 4
        inv = np.float32(theta) ** (-np.arange(freqs, dtype=np.float32) / np.float32(freqs))
        parts.append(np.broadcast_to(inv.astype(np.float32)[:, None], (freqs, 256)))
    return np.concatenate(parts, axis=0)


def rotate(x, cosr, sinr, cosc, sinc):
    f = x.shape[0] // 4
    a, b, c, d = x[:f], x[f : 2 * f], x[2 * f : 3 * f], x[3 * f :]
    return jnp.concatenate(
        [a * cosr - b * sinr, b * cosr + a * sinr, c * cosc - d * sinc, d * cosc + c * sinc], axis=0
    )


def normed_rows(x, gain):
    mean = jnp.mean(x * x, axis=0, keepdims=True)
    return x * lax.rsqrt(mean + eps) * gain


def gain_column(g_ref):
    g = g_ref[...]
    if g.shape[1] == 64:
        g = jnp.concatenate([g, g], axis=1)
    col = jnp.broadcast_to(g, (128, 128)).T
    return jnp.concatenate([col, col], axis=1)


def attention_kernel(
    qn_ref, kn_ref, vn_ref, qb_ref, kb_ref, vb_ref, gqn_ref, gkn_ref, gqb_ref, gkb_ref, inv_ref,
    out_ref,
    kv, qna, qnb, qbt, s_scr, st_m, st_l, on, ob, heads, send_sem, recv_sem, tp_send, tp_recv,
):
    sp = lax.axis_index("sp")
    tp = lax.axis_index("tp")
    me = (sp // 16, (sp // 4) % 4, sp % 4)

    def neighbour(dim, step):
        at = list(me)
        at[dim] = (at[dim] + step + 4) % 4
        return (at[0] * 4 + at[1]) * 4 + at[2]

    barrier = pltpu.get_barrier_semaphore()
    for dim in range(3):
        for step in (1, -1):
            pl.semaphore_signal(barrier, inc=1, device_id=(neighbour(dim, step), tp), device_id_type=MESH)
    pl.semaphore_signal(barrier, inc=1, device_id=(sp, 1 - tp), device_id_type=MESH)

    lane = lax.broadcasted_iota(jnp.int32, (8, 256), 1)
    rows_of = ((lane // 128) + sp * 2).astype(F32)
    cols_of = (lane % 128).astype(F32)

    def tables(first, freqs):
        inv = inv_ref[first : first + freqs, :]
        r = jnp.concatenate([rows_of] * (freqs // 8), axis=0) * inv
        c = jnp.concatenate([cols_of] * (freqs // 8), axis=0) * inv
        return jnp.cos(r), jnp.sin(r), jnp.cos(c), jnp.sin(c)

    tab_n = tables(0, 16)
    tab_b = tables(16, 32)

    kvn = jnp.concatenate([kn_ref[...].astype(F32), vn_ref[...].astype(F32)], axis=1).T
    kt = rotate(normed_rows(kvn[:64], gain_column(gkn_ref)[:64]), *tab_n)
    vt = kvn[64:]
    here = kv.at[me[0], me[1], me[2]]
    here[0:128, :] = jnp.concatenate([kt[:, :128], kt[:, 128:]], axis=0).T.astype(BF)
    here[128:256, :] = jnp.concatenate([vt[:, :128], vt[:, 128:]], axis=0).astype(BF)
    kbt = rotate(normed_rows(kb_ref[...].astype(F32).T, gain_column(gkb_ref)), *tab_b)
    here[256:512, :] = kbt.T.astype(BF)
    vbt = vb_ref[...].astype(F32).T
    here[512:768, :] = jnp.concatenate([vbt[:, :128], vbt[:, 128:]], axis=0).astype(BF)

    pl.semaphore_wait(barrier, 7)

    def part(piece, phase, item, way, mine):
        order = ORDERS[piece]
        at = [me[0], me[1], me[2]]
        rows = pl.ds(piece * 256, 256)
        if phase == 1:
            at[order[0]] = (me[order[0]] + OFFSETS[item] + 4) % 4
        if phase == 2:
            at[order[1]] = (me[order[1]] + OFFSETS[item] + 4) % 4
            at[order[0]] = pl.ds(0, 4)
        back = {0: 0, 1: 0, 2: -1, 3: 1}[way] if mine else {0: -1, 1: 1, 2: -2, 3: 2}[way]
        at[order[phase]] = (me[order[phase]] + back + 4) % 4
        if way >= 2:
            if phase == 2:
                at[order[0]] = pl.ds((way - 2) * 2, 2)
            else:
                rows = pl.ds(piece * 256 + (way - 2) * 128, 128)
        return kv.at[at[0], at[1], at[2], rows]

    def copy_of(piece, phase, item, way, mine):
        ref = part(piece, phase, item, way, mine)
        index = sem_index(piece, phase, item, way)
        to = neighbour(ORDERS[piece][phase], (1, -1, 1, -1)[way])
        return pltpu.make_async_remote_copy(
            src_ref=ref, dst_ref=ref, send_sem=send_sem.at[index], recv_sem=recv_sem.at[index],
            device_id=(to, tp), device_id_type=MESH,
        )

    def send(piece, phase, item):
        copy_of(piece, phase, item, 0, True).start()
        copy_of(piece, phase, item, 1, True).start()

    def arrive(piece, phase, item, way):
        copy_of(piece, phase, item, way, False).wait_recv()
        if way < 2:
            copy_of(piece, phase, item, way + 2, True).start()

    pieces = range(3)
    for p in pieces:
        send(p, 0, 0)
    for p in pieces:
        send(p, 1, 0)

    zero = jnp.zeros((64, 256), BF)
    gq = gain_column(gqn_ref)[:64]
    for pair in range(4):
        qt = qn_ref[:, pair * 128 : pair * 128 + 128].astype(F32).T
        for half in range(2):
            h = pair * 2 + half
            q = rotate(normed_rows(qt[half * 64 : half * 64 + 64], gq), *tab_n).astype(BF)
            q = q.astype(F32) * (64 ** -0.5 * LOG2E)
            hi = q.astype(BF)
            lo = (q - hi.astype(F32)).astype(BF)
            qna[h] = jnp.concatenate([hi, zero, lo, zero], axis=0)
            qnb[h] = jnp.concatenate([zero, hi, zero, lo], axis=0)
    gq = gain_column(gqb_ref)
    for h in range(4):
        qt = qb_ref[:, h * 128 : h * 128 + 128].astype(F32).T
        q = rotate(normed_rows(qt, gq), *tab_b).astype(BF)
        q = q.astype(F32) * (128 ** -0.5 * LOG2E)
        hi = q.astype(BF)
        lo = (q - hi.astype(F32)).astype(BF)
        qbt[h] = jnp.concatenate([hi, lo], axis=0)

    st_m[...] = jnp.full(st_m.shape, -1e30, F32)
    st_l[...] = jnp.zeros(st_l.shape, F32)
    on[...] = jnp.zeros(on.shape, F32)
    ob[...] = jnp.zeros(ob.shape, F32)

    def qk(t, zz, yy, slot):
        mx = None
        for u in range(NB):
            if t < 8:
                k = kv[zz, yy, u, 0:128, :]
                k2 = jnp.concatenate([k, k], axis=1)
                sa = jnp.dot(k2, qna[t], preferred_element_type=F32)
                sb = jnp.dot(k2, qnb[t], preferred_element_type=F32)
                s = jnp.concatenate([sa, sb], axis=0)
            else:
                k = kv[zz, yy, u, 256:512, :]
                k2 = jnp.concatenate([k, k], axis=1)
                s = jnp.dot(k2, qbt[t - 8], preferred_element_type=F32)
            s_scr[slot, pl.ds(u * 256, 256), :] = s
            r = jnp.max(s.reshape(32, 8, 256), axis=0)
            mx = r if mx is None else jnp.maximum(mx, r)
        return mx

    def pv(t, zz, yy, slot, mx):
        m_old = st_m[t]
        mm = jnp.max(jnp.maximum(mx, m_old), axis=0, keepdims=True)
        alpha = jnp.exp2(m_old[0:1] - mm)
        ps, vs, ls = [], [], None
        for u in range(NB):
            p = jnp.exp2(s_scr[slot, pl.ds(u * 256, 256), :] - mm)
            l = jnp.sum(p.reshape(32, 8, 256), axis=0)
            ls = l if ls is None else ls + l
            ps.append(p.astype(BF))
            if t < 8:
                vs.append(kv[zz, yy, u, 128:192, :])
                vs.append(kv[zz, yy, u, 192:256, :])
            else:
                vs.append(kv[zz, yy, u, 512:640, :])
                vs.append(kv[zz, yy, u, 640:768, :])
        o = jnp.dot(jnp.concatenate(vs, axis=1), jnp.concatenate(ps, axis=0), preferred_element_type=F32)
        st_m[t] = jnp.broadcast_to(mm, (8, 256))
        st_l[t] = st_l[t] * alpha + ls
        if t < 8:
            on[t] = on[t] * alpha + o
        else:
            ob[t - 8] = ob[t - 8] * alpha + o

    def block(first, last, zz, yy):
        mx = qk(first, zz, yy, 0)
        for t in range(first, last):
            slot = (t - first) % 2
            nx = qk(t + 1, zz, yy, 1 - slot) if t + 1 < last else None
            pv(t, zz, yy, slot, mx)
            mx = nx

    def opening():
        for p in pieces:
            arrive(p, 0, 0, 0)
            arrive(p, 0, 0, 1)
            send(p, 1, 1)
            send(p, 1, 2)
        for p in pieces:
            arrive(p, 1, 0, 0)
            arrive(p, 1, 0, 1)
        for p in pieces:
            arrive(p, 0, 0, 2)
            arrive(p, 0, 0, 3)
            send(p, 1, 3)
            send(p, 2, 0)

    def second():
        for item in (1, 2):
            for p in pieces:
                arrive(p, 1, item, 0)
                arrive(p, 1, item, 1)
        for p in pieces:
            arrive(p, 1, 3, 0)
            arrive(p, 1, 3, 1)
            send(p, 2, 1)
            send(p, 2, 2)

    def third():
        for p in pieces:
            for item in range(4):
                arrive(p, 1, item, 2)
                arrive(p, 1, item, 3)
            send(p, 2, 3)

    def sides(item):
        for p in pieces:
            arrive(p, 2, item, 0)
            arrive(p, 2, item, 1)

    def far(item):
        for p in pieces:
            arrive(p, 2, item, 2)
            arrive(p, 2, item, 3)

    events = {1: second, 3: third}
    for k in range(4):
        events[4 + 2 * k] = functools.partial(sides, k)
        events[12 + k] = functools.partial(far, k)

    def chunk_offset(c):
        return (c % 2) * 3 * (1 - c // 2) + (c // 2) * (1 + c % 2)

    def narrow_round(i, _):
        for at, event in events.items():
            pl.when(i == at)(event)
        early = 1 - jnp.minimum(i // 4, 1)
        late = i // 12
        middle = 1 - early - late
        k = i - 4
        c = early * i + middle * (k // 2) + late * (i - 12)
        zo = middle * (3 - 2 * (k % 2)) + late * 2
        zz = (me[0] + zo) % 4
        yy = (me[1] + chunk_offset(c)) % 4
        block(0, 8, zz, yy)
        return 0

    def broad_round(i, _):
        block(8, 12, i // 4, i % 4)
        return 0

    opening()
    lax.fori_loop(0, 16, narrow_round, 0)
    lax.fori_loop(0, 16, broad_round, 0)

    for pair in range(4):
        cols = []
        for t in (2 * pair, 2 * pair + 1):
            cols.append(on[t] / jnp.sum(st_l[t], axis=0, keepdims=True))
        heads[:, pair * 128 : pair * 128 + 128] = jnp.concatenate(cols, axis=0).T.astype(BF)
    for t in range(4):
        o = ob[t] / jnp.sum(st_l[8 + t], axis=0, keepdims=True)
        heads[:, 512 + t * 128 : 640 + t * 128] = o.T.astype(BF)

    mine = pl.ds(pl.multiple_of(tp * 128, 128), 128)
    other = pl.ds(pl.multiple_of((1 - tp) * 128, 128), 128)
    swaps = []
    for g in range(2):
        place = pl.ds(pl.multiple_of(g * 1024 + tp * 512, 128), 512)
        swap = pltpu.make_async_remote_copy(
            src_ref=heads.at[other, pl.ds(g * 512, 512)], dst_ref=out_ref.at[:, place],
            send_sem=tp_send.at[g], recv_sem=tp_recv.at[g], device_id=(sp, 1 - tp), device_id_type=MESH,
        )
        swap.start()
        swaps.append(swap)
        out_ref[:, place] = heads[mine, pl.ds(g * 512, 512)]
    for p in pieces:
        for phase in range(3):
            for item in range(1 if phase == 0 else 4):
                for way in range(4):
                    copy_of(p, phase, item, way, True).wait_send()
    for g in range(2):
        place = pl.ds(pl.multiple_of(g * 1024 + (1 - tp) * 512, 128), 512)
        pltpu.make_async_remote_copy(
            src_ref=heads.at[other, pl.ds(g * 512, 512)], dst_ref=out_ref.at[:, place],
            send_sem=tp_send.at[g], recv_sem=tp_recv.at[g], device_id=(sp, 1 - tp), device_id_type=MESH,
        ).wait_recv()
        swaps[g].wait_send()


def attention(qn, kn, vn, qb, kb, vb, gqn, gkn, gqb, gkb):
    inv = jnp.asarray(inverse_table())
    vm = pl.BlockSpec(memory_space=pltpu.VMEM)
    return pl.pallas_call(
        attention_kernel,
        out_shape=jax.ShapeDtypeStruct((128, 2048), BF),
        in_specs=[vm] * 11,
        out_specs=vm,
        scratch_shapes=[
            pltpu.VMEM((4, 4, 4, 768, 128), BF),
            pltpu.VMEM((8, 256, 256), BF),
            pltpu.VMEM((8, 256, 256), BF),
            pltpu.VMEM((4, 256, 256), BF),
            pltpu.VMEM((2, NB * 256, 256), F32),
            pltpu.VMEM((12, 8, 256), F32),
            pltpu.VMEM((12, 8, 256), F32),
            pltpu.VMEM((8, 64, 256), F32),
            pltpu.VMEM((4, 128, 256), F32),
            pltpu.VMEM((256, 1024), BF),
            pltpu.SemaphoreType.DMA((108,)),
            pltpu.SemaphoreType.DMA((108,)),
            pltpu.SemaphoreType.DMA((2,)),
            pltpu.SemaphoreType.DMA((2,)),
        ],
        compiler_params=pltpu.CompilerParams(
            collective_id=0, has_side_effects=True, vmem_limit_bytes=60 * 1024 * 1024
        ),
        name="attention",
    )(
        qn, kn, vn, qb, kb, vb,
        gqn.reshape(1, -1), gkn.reshape(1, -1), gqb.reshape(1, -1), gkb.reshape(1, -1), inv,
    )


def cut_along(value, dim, size):
    before, after = (value.shape[:dim], value.shape[dim + 1 :])
    return jnp.moveaxis(value.reshape(*before, size, -1, *after), dim, 0)


def summed_on_arrival(value, axis, dim):
    size = lax.axis_size(axis)
    blocks = lax.all_to_all(cut_along(value, dim, size), axis, 0, 0, tiled=True)
    return jnp.sum(blocks.astype(jnp.float32), axis=0)


def joined_along(blocks, dim):
    shape = list(blocks.shape[1:])
    shape[dim] *= blocks.shape[0]
    return jnp.moveaxis(blocks, 0, dim).reshape(shape)


def copy_for_each(value, axis):
    size = lax.axis_size(axis)
    return lax.all_to_all(
        jnp.broadcast_to(value[None], (size, *value.shape)), axis, 0, 0, tiled=True
    )


def gather_directly(value, axis, dim):
    return joined_along(copy_for_each(value, axis), dim)


def local(
    stream,
    query_narrow,
    key_narrow,
    value_narrow,
    query_broad,
    key_broad,
    value_broad,
    narrow_query_gain,
    narrow_key_gain,
    broad_query_gain,
    broad_key_gain,
    out_weight,
    norm_gain,
    gate_weight,
    up_weight,
    down_weight,
    route_ids,
    route_weights,
):
    heads = attention(
        query_narrow, key_narrow, value_narrow, query_broad, key_broad, value_broad,
        narrow_query_gain, narrow_key_gain, broad_query_gain, broad_key_gain,
    )
    mixed = jnp.dot(heads, out_weight, preferred_element_type=jnp.float32)
    wide = (stream.astype(jnp.float32) + mixed).astype(jnp.bfloat16).astype(jnp.float32)
    normed = (
        wide * lax.rsqrt(jnp.mean(wide * wide, axis=-1, keepdims=True) + eps) * norm_gain
    ).astype(jnp.bfloat16)
    tokens_here, topk = route_ids.shape
    width_model = normed.shape[1]
    experts = lax.axis_size("sp")
    capacity = (2 * tokens_here * topk + experts - 1) // experts
    flat = route_ids.reshape(-1)
    hits = (flat[:, None] == jnp.arange(experts, dtype=jnp.int32)[None, :]).astype(jnp.int32)
    ranks = jnp.sum((jnp.cumsum(hits, axis=0) - 1) * hits, axis=1)
    slots = flat * capacity + ranks
    table = (jnp.arange(experts * capacity, dtype=jnp.int32)[:, None] == slots[None, :]).astype(
        jnp.bfloat16
    )
    table = jnp.sum(table.reshape(experts * capacity, tokens_here, topk), axis=2)
    sent = jnp.dot(table, normed, preferred_element_type=jnp.float32).astype(jnp.bfloat16)
    sent = sent.reshape(experts, capacity, width_model)
    piece = gather_directly(
        lax.all_to_all(sent, "sp", split_axis=0, concat_axis=0, tiled=True), "tp", 0
    )
    rows = piece.reshape(-1, piece.shape[-1])
    gate = jnp.dot(rows, gate_weight[0], preferred_element_type=jnp.float32)
    upper = jnp.dot(rows, up_weight[0], preferred_element_type=jnp.float32)
    hidden = (jax.nn.silu(gate) * upper).astype(jnp.bfloat16)
    partial_out = jnp.dot(hidden, down_weight[0], preferred_element_type=jnp.float32).astype(
        jnp.bfloat16
    )
    terms = lax.optimization_barrier(partial_out).astype(jnp.float32).reshape(piece.shape)
    summed = summed_on_arrival(terms.astype(jnp.bfloat16), "tp", 0).astype(jnp.bfloat16)
    back = lax.all_to_all(summed, "sp", split_axis=0, concat_axis=0, tiled=True)
    picked = jnp.take(back.reshape(experts * capacity, width_model), slots, axis=0)
    picked = picked.astype(jnp.float32).reshape(tokens_here, topk, width_model)
    routed = jnp.sum(picked * route_weights[..., None], axis=1)
    return (wide + routed).astype(jnp.bfloat16)


def solution(mesh):
    return jax.shard_map(
        local,
        mesh=mesh,
        in_specs=(
            P(("sp", "tp"), None),
            P("sp", "tp"),
            P("sp", "tp"),
            P("sp", "tp"),
            P("sp", "tp"),
            P("sp", "tp"),
            P("sp", "tp"),
            P(),
            P(),
            P(),
            P(),
            P(),
            P(),
            P("sp", None, "tp"),
            P("sp", None, "tp"),
            P("sp", "tp", None),
            P(("sp", "tp"), None),
            P(("sp", "tp"), None),
        ),
        out_specs=P(("sp", "tp"), None),
        check_vma=False,
    )
```

```python
import functools
import math

import jax
import jax.numpy as jnp
import numpy as np
from jax import lax
from jax.experimental import pallas as pl
from jax.experimental.pallas import tpu as pltpu
from jax.sharding import PartitionSpec as P

F32 = jnp.float32
BF = jnp.bfloat16
MESH = pl.DeviceIdType.MESH
eps = 1e-06
theta = 10000.0
LOG2E = math.log2(math.e)
NB = 4
ORDERS = ((2, 1, 0), (1, 0, 2), (0, 2, 1))
OFFSETS = (0, -1, 1, 2)


def far_first():
    offs = [(a, b, c) for a in range(4) for b in range(4) for c in range(4) if a + b + c > 0]
    seen, groups = set(), []
    for o in offs:
        if o in seen:
            continue
        orbit = []
        for r in (o, (o[1], o[2], o[0]), (o[2], o[0], o[1])):
            for s in (r, tuple((-v) % 4 for v in r)):
                if s not in orbit:
                    orbit.append(s)
        seen.update(orbit)
        groups.append(orbit)
    groups.sort(key=lambda g: -sum(min(v, 4 - v) for v in g[0]))
    return [o for g in groups for o in g]


PEERS = far_first()


def sem_index(piece, phase, item, way):
    base = (0, 4, 20)[phase]
    return piece * 36 + base + item * 4 + way


def inverse_table():
    parts = []
    for dim in (64, 128):
        freqs = dim // 4
        inv = np.float32(theta) ** (-np.arange(freqs, dtype=np.float32) / np.float32(freqs))
        parts.append(np.broadcast_to(inv.astype(np.float32)[:, None], (freqs, 256)))
    return np.concatenate(parts, axis=0)


def rotate(x, cosr, sinr, cosc, sinc):
    f = x.shape[0] // 4
    a, b, c, d = x[:f], x[f : 2 * f], x[2 * f : 3 * f], x[3 * f :]
    return jnp.concatenate(
        [a * cosr - b * sinr, b * cosr + a * sinr, c * cosc - d * sinc, d * cosc + c * sinc], axis=0
    )


def normed_rows(x, gain):
    mean = jnp.mean(x * x, axis=0, keepdims=True)
    return x * lax.rsqrt(mean + eps) * gain


def gain_column(g_ref):
    g = g_ref[...]
    if g.shape[1] == 64:
        g = jnp.concatenate([g, g], axis=1)
    col = jnp.broadcast_to(g, (128, 128)).T
    return jnp.concatenate([col, col], axis=1)


def layer_kernel(
    qn_ref, kn_ref, vn_ref, qb_ref, kb_ref, vb_ref, gqn_ref, gkn_ref, gqb_ref, gkb_ref, inv_ref,
    stream_ref, ngain_ref, ids_ref, rw_ref, ow_hbm, gw_hbm, uw_hbm, dw_hbm,
    out_ref,
    kv, qna, qnb, qbt, s_scr, st_m, st_l, on, ob, heads, full, ow, gw, uw, dw, wide, normed,
    table, comb, sent, got, got2, part_a, part_b, part_c, ret, back,
    send_sem, recv_sem, tp_send, tp_recv, load_sem, d_send, d_recv, r_send, r_recv,
    f_send, f_recv, p_send, p_recv,
):
    sp = lax.axis_index("sp")
    tp = lax.axis_index("tp")
    me = (sp // 16, (sp // 4) % 4, sp % 4)

    def neighbour(dim, step):
        at = list(me)
        at[dim] = (at[dim] + step + 4) % 4
        return (at[0] * 4 + at[1]) * 4 + at[2]

    def chip_at(offset, sign):
        at = [(me[d] + sign * offset[d] + 4) % 4 for d in range(3)]
        return (at[0] * 4 + at[1]) * 4 + at[2]

    barrier = pltpu.get_barrier_semaphore()
    for o in PEERS:
        pl.semaphore_signal(barrier, inc=1, device_id=(chip_at(o, 1), tp), device_id_type=MESH)
    pl.semaphore_signal(barrier, inc=1, device_id=(sp, 1 - tp), device_id_type=MESH)

    loads = [
        pltpu.make_async_copy(ow_hbm, ow, load_sem.at[0]),
        pltpu.make_async_copy(gw_hbm.at[0], gw, load_sem.at[1]),
        pltpu.make_async_copy(uw_hbm.at[0], uw, load_sem.at[2]),
        pltpu.make_async_copy(dw_hbm.at[0], dw, load_sem.at[3]),
    ]
    for load in loads:
        load.start()

    lane = lax.broadcasted_iota(jnp.int32, (8, 256), 1)
    rows_of = ((lane // 128) + sp * 2).astype(F32)
    cols_of = (lane % 128).astype(F32)

    def tables(first, freqs):
        inv = inv_ref[first : first + freqs, :]
        r = jnp.concatenate([rows_of] * (freqs // 8), axis=0) * inv
        c = jnp.concatenate([cols_of] * (freqs // 8), axis=0) * inv
        return jnp.cos(r), jnp.sin(r), jnp.cos(c), jnp.sin(c)

    tab_n = tables(0, 16)
    tab_b = tables(16, 32)

    kt = rotate(normed_rows(kn_ref[...].astype(F32), gain_column(gkn_ref)[:64]), *tab_n)
    vt = vn_ref[...]
    here = kv.at[me[0], me[1], me[2]]
    here[0:128, :] = jnp.concatenate([kt[:, :128], kt[:, 128:]], axis=0).T.astype(BF)
    here[128:256, :] = jnp.concatenate([vt[:, :128], vt[:, 128:]], axis=0)
    kbt = rotate(normed_rows(kb_ref[...].astype(F32).T, gain_column(gkb_ref)), *tab_b)
    here[256:512, :] = kbt.T.astype(BF)
    vbt = vb_ref[...].astype(F32).T
    here[512:768, :] = jnp.concatenate([vbt[:, :128], vbt[:, 128:]], axis=0).astype(BF)

    pl.semaphore_wait(barrier, 64)

    def part(piece, phase, item, way, mine):
        order = ORDERS[piece]
        at = [me[0], me[1], me[2]]
        rows = pl.ds(piece * 256, 256)
        if phase == 1:
            at[order[0]] = (me[order[0]] + OFFSETS[item] + 4) % 4
        if phase == 2:
            at[order[1]] = (me[order[1]] + OFFSETS[item] + 4) % 4
            at[order[0]] = pl.ds(0, 4)
        back = {0: 0, 1: 0, 2: -1, 3: 1}[way] if mine else {0: -1, 1: 1, 2: -2, 3: 2}[way]
        at[order[phase]] = (me[order[phase]] + back + 4) % 4
        if way >= 2:
            if phase == 2:
                at[order[0]] = pl.ds((way - 2) * 2, 2)
            else:
                rows = pl.ds(piece * 256 + (way - 2) * 128, 128)
        return kv.at[at[0], at[1], at[2], rows]

    def copy_of(piece, phase, item, way, mine):
        ref = part(piece, phase, item, way, mine)
        index = sem_index(piece, phase, item, way)
        to = neighbour(ORDERS[piece][phase], (1, -1, 1, -1)[way])
        return pltpu.make_async_remote_copy(
            src_ref=ref, dst_ref=ref, send_sem=send_sem.at[index], recv_sem=recv_sem.at[index],
            device_id=(to, tp), device_id_type=MESH,
        )

    def send(piece, phase, item):
        copy_of(piece, phase, item, 0, True).start()
        copy_of(piece, phase, item, 1, True).start()

    def arrive(piece, phase, item, way):
        copy_of(piece, phase, item, way, False).wait_recv()
        if way < 2:
            copy_of(piece, phase, item, way + 2, True).start()

    pieces = range(3)
    for p in pieces:
        send(p, 0, 0)
    for p in pieces:
        send(p, 1, 0)

    zero = jnp.zeros((64, 256), BF)
    gq = gain_column(gqn_ref)[:64]
    for pair in range(4):
        qt = qn_ref[:, pair * 128 : pair * 128 + 128].astype(F32).T
        for half in range(2):
            h = pair * 2 + half
            q = rotate(normed_rows(qt[half * 64 : half * 64 + 64], gq), *tab_n).astype(BF)
            q = q.astype(F32) * (64 ** -0.5 * LOG2E)
            hi = q.astype(BF)
            lo = (q - hi.astype(F32)).astype(BF)
            qna[h] = jnp.concatenate([hi, zero, lo, zero], axis=0)
            qnb[h] = jnp.concatenate([zero, hi, zero, lo], axis=0)
    gq = gain_column(gqb_ref)
    for h in range(4):
        qt = qb_ref[:, h * 128 : h * 128 + 128].astype(F32).T
        q = rotate(normed_rows(qt, gq), *tab_b).astype(BF)
        q = q.astype(F32) * (128 ** -0.5 * LOG2E)
        hi = q.astype(BF)
        lo = (q - hi.astype(F32)).astype(BF)
        qbt[h] = jnp.concatenate([hi, lo], axis=0)

    slot = lax.broadcasted_iota(jnp.int32, (512, 128), 0)
    expert = slot // 8
    ids = ids_ref[...]
    first = expert == ids[0:1]
    second_ = expert == ids[1:2]
    hits = jnp.where(jnp.logical_or(first, second_), 1.0, 0.0)
    before = lax.broadcasted_iota(jnp.int32, (128, 128), 0) < lax.broadcasted_iota(jnp.int32, (128, 128), 1)
    ranks = jnp.dot(hits.astype(BF), jnp.where(before, 1.0, 0.0).astype(BF), preferred_element_type=F32)
    chosen = jnp.where(ranks == (slot % 8).astype(F32), hits, 0.0)
    table[...] = chosen.astype(BF)
    rw = rw_ref[...]
    weight = (chosen * (jnp.where(first, rw[0:1], 0.0) + jnp.where(second_, rw[1:2], 0.0))).T
    weight_hi = weight.astype(BF)
    comb[:, 0:512] = weight_hi
    comb[:, 512:1024] = (weight - weight_hi.astype(F32)).astype(BF)

    st_m[...] = jnp.full(st_m.shape, -1e30, F32)
    st_l[...] = jnp.zeros(st_l.shape, F32)
    on[...] = jnp.zeros(on.shape, F32)
    ob[...] = jnp.zeros(ob.shape, F32)

    def qk(t, zz, yy, slot):
        mx = None
        for u in range(NB):
            if t < 8:
                k = kv[zz, yy, u, 0:128, :]
                k2 = jnp.concatenate([k, k], axis=1)
                sa = jnp.dot(k2, qna[t], preferred_element_type=F32)
                sb = jnp.dot(k2, qnb[t], preferred_element_type=F32)
                s = jnp.concatenate([sa, sb], axis=0)
            else:
                k = kv[zz, yy, u, 256:512, :]
                k2 = jnp.concatenate([k, k], axis=1)
                s = jnp.dot(k2, qbt[t - 8], preferred_element_type=F32)
            s_scr[slot, pl.ds(u * 256, 256), :] = s
            r = jnp.max(s.reshape(32, 8, 256), axis=0)
            mx = r if mx is None else jnp.maximum(mx, r)
        return mx

    def pv(t, zz, yy, slot, mx):
        m_old = st_m[t]
        mm = jnp.max(jnp.maximum(mx, m_old), axis=0, keepdims=True)
        alpha = jnp.exp2(m_old[0:1] - mm)
        ps, vs, ls = [], [], None
        for u in range(NB):
            p = jnp.exp2(s_scr[slot, pl.ds(u * 256, 256), :] - mm)
            l = jnp.sum(p.reshape(32, 8, 256), axis=0)
            ls = l if ls is None else ls + l
            ps.append(p.astype(BF))
            if t < 8:
                vs.append(kv[zz, yy, u, 128:192, :])
                vs.append(kv[zz, yy, u, 192:256, :])
            else:
                vs.append(kv[zz, yy, u, 512:640, :])
                vs.append(kv[zz, yy, u, 640:768, :])
        o = jnp.dot(jnp.concatenate(vs, axis=1), jnp.concatenate(ps, axis=0), preferred_element_type=F32)
        st_m[t] = jnp.broadcast_to(mm, (8, 256))
        st_l[t] = st_l[t] * alpha + ls
        if t < 8:
            on[t] = on[t] * alpha + o
        else:
            ob[t - 8] = ob[t - 8] * alpha + o

    def block(first, last, zz, yy):
        mx = qk(first, zz, yy, 0)
        for t in range(first, last):
            slot = (t - first) % 2
            nx = qk(t + 1, zz, yy, 1 - slot) if t + 1 < last else None
            pv(t, zz, yy, slot, mx)
            mx = nx

    def opening():
        for p in pieces:
            arrive(p, 0, 0, 0)
            arrive(p, 0, 0, 1)
            send(p, 1, 1)
            send(p, 1, 2)
        for p in pieces:
            arrive(p, 1, 0, 0)
            arrive(p, 1, 0, 1)
        for p in pieces:
            arrive(p, 0, 0, 2)
            arrive(p, 0, 0, 3)
            send(p, 1, 3)
            send(p, 2, 0)

    def second():
        for item in (1, 2):
            for p in pieces:
                arrive(p, 1, item, 0)
                arrive(p, 1, item, 1)
        for p in pieces:
            arrive(p, 1, 3, 0)
            arrive(p, 1, 3, 1)
            send(p, 2, 1)
            send(p, 2, 2)

    def third():
        for p in pieces:
            for item in range(4):
                arrive(p, 1, item, 2)
                arrive(p, 1, item, 3)
            send(p, 2, 3)

    def sides(item):
        for p in pieces:
            arrive(p, 2, item, 0)
            arrive(p, 2, item, 1)

    def far(item):
        for p in pieces:
            arrive(p, 2, item, 2)
            arrive(p, 2, item, 3)

    events = {1: second, 3: third}
    for k in range(4):
        events[4 + 2 * k] = functools.partial(sides, k)
        events[12 + k] = functools.partial(far, k)

    def chunk_offset(c):
        return (c % 2) * 3 * (1 - c // 2) + (c // 2) * (1 + c % 2)

    def narrow_round(i, _):
        for at, event in events.items():
            pl.when(i == at)(event)
        early = 1 - jnp.minimum(i // 4, 1)
        late = i // 12
        middle = 1 - early - late
        k = i - 4
        c = early * i + middle * (k // 2) + late * (i - 12)
        zo = middle * (3 - 2 * (k % 2)) + late * 2
        zz = (me[0] + zo) % 4
        yy = (me[1] + chunk_offset(c)) % 4
        block(0, 8, zz, yy)
        return 0

    def broad_round(i, _):
        block(8, 12, i // 4, i % 4)
        return 0

    opening()
    lax.fori_loop(0, 16, narrow_round, 0)
    lax.fori_loop(0, 16, broad_round, 0)

    for pair in range(4):
        cols = []
        for t in (2 * pair, 2 * pair + 1):
            cols.append(on[t] / jnp.sum(st_l[t], axis=0, keepdims=True))
        heads[:, pair * 128 : pair * 128 + 128] = jnp.concatenate(cols, axis=0).T.astype(BF)
    for t in range(4):
        o = ob[t] / jnp.sum(st_l[8 + t], axis=0, keepdims=True)
        heads[:, 512 + t * 128 : 640 + t * 128] = o.T.astype(BF)

    mine = pl.ds(pl.multiple_of(tp * 128, 128), 128)
    other = pl.ds(pl.multiple_of((1 - tp) * 128, 128), 128)
    swaps = []
    for g in range(2):
        place = pl.ds(pl.multiple_of(g * 1024 + tp * 512, 128), 512)
        swap = pltpu.make_async_remote_copy(
            src_ref=heads.at[other, pl.ds(g * 512, 512)], dst_ref=full.at[:, place],
            send_sem=tp_send.at[g], recv_sem=tp_recv.at[g], device_id=(sp, 1 - tp), device_id_type=MESH,
        )
        swap.start()
        swaps.append(swap)
        full[:, place] = heads[mine, pl.ds(g * 512, 512)]
    for g in range(2):
        place = pl.ds(pl.multiple_of(g * 1024 + (1 - tp) * 512, 128), 512)
        pltpu.make_async_remote_copy(
            src_ref=heads.at[other, pl.ds(g * 512, 512)], dst_ref=full.at[:, place],
            send_sem=tp_send.at[g], recv_sem=tp_recv.at[g], device_id=(sp, 1 - tp), device_id_type=MESH,
        ).wait_recv()
        swaps[g].wait_send()

    for load in loads:
        load.wait()
    squares = jnp.zeros((128, 128), F32)
    for b in range(4):
        cols = slice(b * 512, b * 512 + 512)
        m = jnp.dot(full[...], ow[:, cols], preferred_element_type=F32)
        m = (stream_ref[:, cols].astype(F32) + m).astype(BF)
        wide[:, cols] = m
        m = m.astype(F32)
        m = m * m
        squares = squares + ((m[:, 0:128] + m[:, 128:256]) + (m[:, 256:384] + m[:, 384:512]))
    scale = lax.rsqrt(jnp.sum(squares, axis=1, keepdims=True) / 2048 + eps)
    for b in range(4):
        cols = slice(b * 512, b * 512 + 512)
        normed[:, cols] = (wide[:, cols].astype(F32) * scale * ngain_ref[:, cols]).astype(BF)

    for b in range(8):
        cols = slice(b * 256, b * 256 + 256)
        rows = jnp.dot(table[...], normed[:, cols], preferred_element_type=F32)
        sent[:, :, cols] = rows.reshape(64, 8, 256).astype(BF)

    def dispatch(n):
        to = chip_at(PEERS[n], 1)
        return pltpu.make_async_remote_copy(
            src_ref=sent.at[to], dst_ref=got.at[n], send_sem=d_send.at[n], recv_sem=d_recv.at[n],
            device_id=(to, tp), device_id_type=MESH,
        )

    def giveback(n):
        to = chip_at(PEERS[n], -1)
        return pltpu.make_async_remote_copy(
            src_ref=ret.at[n], dst_ref=back.at[sp], send_sem=r_send.at[n], recv_sem=r_recv.at[n],
            device_id=(to, tp), device_id_type=MESH,
        )

    def given(n):
        at = chip_at(PEERS[n], 1)
        return pltpu.make_async_remote_copy(
            src_ref=ret.at[n], dst_ref=back.at[at], send_sem=r_send.at[n], recv_sem=r_recv.at[n],
            device_id=(at, tp), device_id_type=MESH,
        )

    for n in range(63):
        dispatch(n).start()
    got[63] = sent[sp]

    def forward(c):
        rows = pl.ds(c * 16, 16)
        return pltpu.make_async_remote_copy(
            src_ref=got.at[rows], dst_ref=got2.at[rows], send_sem=f_send.at[c], recv_sem=f_recv.at[c],
            device_id=(sp, 1 - tp), device_id_type=MESH,
        )

    def partial(c):
        return pltpu.make_async_remote_copy(
            src_ref=part_b.at[c], dst_ref=part_c.at[c], send_sem=p_send.at[c], recv_sem=p_recv.at[c],
            device_id=(sp, 1 - tp), device_id_type=MESH,
        )

    for c in range(4):
        members = [n for n in range(c * 16, c * 16 + 16) if n < 63]
        for n in members:
            dispatch(n).wait_recv()
        forward(c).start()
        forward(c).wait_recv()
        rows = jnp.concatenate(
            [got[c * 16 : c * 16 + 16].reshape(128, 2048), got2[c * 16 : c * 16 + 16].reshape(128, 2048)], axis=0
        )
        gate = jnp.dot(rows, gw[...], preferred_element_type=F32)
        upper = jnp.dot(rows, uw[...], preferred_element_type=F32)
        hidden = (gate / (1.0 + jnp.exp(-gate)) * upper).astype(BF)
        for b in range(4):
            cols = slice(b * 512, b * 512 + 512)
            piece = jnp.dot(hidden, dw[:, cols], preferred_element_type=F32).astype(BF)
            part_a[:, cols] = piece[:128]
            part_b[c, :, cols] = piece[128:]
        partial(c).start()
        partial(c).wait_recv()
        total = (part_a[...].astype(F32) + part_c[c].astype(F32)).astype(BF)
        ret[c * 16 : c * 16 + 16] = total.reshape(16, 8, 2048)
        for n in members:
            giveback(n).start()
    back[sp] = ret[63]
    for n in range(63):
        given(n).wait_recv()
    rows = back[...].reshape(512, 2048)
    for b in range(4):
        cols = slice(b * 512, b * 512 + 512)
        piece = rows[:, cols]
        routed = jnp.dot(comb[...], jnp.concatenate([piece, piece], axis=0), preferred_element_type=F32)
        out_ref[:, cols] = (wide[:, cols].astype(F32) + routed).astype(BF)
    for n in range(63):
        dispatch(n).wait_send()
        giveback(n).wait_send()
    for c in range(4):
        forward(c).wait_send()
        partial(c).wait_send()
    for p in pieces:
        for phase in range(3):
            for item in range(1 if phase == 0 else 4):
                for way in range(4):
                    copy_of(p, phase, item, way, True).wait_send()


def layer(
    stream, qn, kn, vn, qb, kb, vb, gqn, gkn, gqb, gkb, ow, ngain, gw, uw, dw, route_ids, route_weights
):
    inv = jnp.asarray(inverse_table())
    vm = pl.BlockSpec(memory_space=pltpu.VMEM)
    return pl.pallas_call(
        layer_kernel,
        out_shape=jax.ShapeDtypeStruct((128, 2048), BF),
        in_specs=[vm] * 15 + [pl.BlockSpec(memory_space=pl.ANY)] * 4,
        out_specs=vm,
        scratch_shapes=[
            pltpu.VMEM((4, 4, 4, 768, 128), BF),
            pltpu.VMEM((8, 256, 256), BF),
            pltpu.VMEM((8, 256, 256), BF),
            pltpu.VMEM((4, 256, 256), BF),
            pltpu.VMEM((2, NB * 256, 256), F32),
            pltpu.VMEM((12, 8, 256), F32),
            pltpu.VMEM((12, 8, 256), F32),
            pltpu.VMEM((8, 64, 256), F32),
            pltpu.VMEM((4, 128, 256), F32),
            pltpu.VMEM((256, 1024), BF),
            pltpu.VMEM((128, 2048), BF),
            pltpu.VMEM((2048, 2048), BF),
            pltpu.VMEM((2048, 512), BF),
            pltpu.VMEM((2048, 512), BF),
            pltpu.VMEM((512, 2048), BF),
            pltpu.VMEM((128, 2048), BF),
            pltpu.VMEM((128, 2048), BF),
            pltpu.VMEM((512, 128), BF),
            pltpu.VMEM((128, 1024), BF),
            pltpu.VMEM((64, 8, 2048), BF),
            pltpu.VMEM((64, 8, 2048), BF),
            pltpu.VMEM((64, 8, 2048), BF),
            pltpu.VMEM((128, 2048), BF),
            pltpu.VMEM((4, 128, 2048), BF),
            pltpu.VMEM((4, 128, 2048), BF),
            pltpu.VMEM((64, 8, 2048), BF),
            pltpu.VMEM((64, 8, 2048), BF),
            pltpu.SemaphoreType.DMA((108,)),
            pltpu.SemaphoreType.DMA((108,)),
            pltpu.SemaphoreType.DMA((2,)),
            pltpu.SemaphoreType.DMA((2,)),
            pltpu.SemaphoreType.DMA((4,)),
            pltpu.SemaphoreType.DMA((63,)),
            pltpu.SemaphoreType.DMA((63,)),
            pltpu.SemaphoreType.DMA((63,)),
            pltpu.SemaphoreType.DMA((63,)),
            pltpu.SemaphoreType.DMA((4,)),
            pltpu.SemaphoreType.DMA((4,)),
            pltpu.SemaphoreType.DMA((4,)),
            pltpu.SemaphoreType.DMA((4,)),
        ],
        compiler_params=pltpu.CompilerParams(
            collective_id=0, has_side_effects=True, vmem_limit_bytes=67043328
        ),
        name="layer",
    )(
        qn, kn.T, vn.T, qb, kb, vb,
        gqn.reshape(1, -1), gkn.reshape(1, -1), gqb.reshape(1, -1), gkb.reshape(1, -1), inv,
        stream, ngain.reshape(1, -1), route_ids.T, route_weights.T, ow, gw, uw, dw,
    )


def solution(mesh):
    return jax.shard_map(
        layer,
        mesh=mesh,
        in_specs=(
            P(("sp", "tp"), None),
            P("sp", "tp"),
            P("sp", "tp"),
            P("sp", "tp"),
            P("sp", "tp"),
            P("sp", "tp"),
            P("sp", "tp"),
            P(),
            P(),
            P(),
            P(),
            P(),
            P(),
            P("sp", None, "tp"),
            P("sp", None, "tp"),
            P("sp", "tp", None),
            P(("sp", "tp"), None),
            P(("sp", "tp"), None),
        ),
        out_specs=P(("sp", "tp"), None),
        check_vma=False,
    )
```

```python
import functools
import math

import jax
import jax.numpy as jnp
import numpy as np
from jax import lax
from jax.experimental import pallas as pl
from jax.experimental.pallas import tpu as pltpu
from jax.sharding import PartitionSpec as P

F32 = jnp.float32
BF = jnp.bfloat16
MESH = pl.DeviceIdType.MESH
eps = 1e-06
theta = 10000.0
LOG2E = math.log2(math.e)
ORDERS = ((2, 1, 0), (1, 0, 2), (0, 2, 1))
OFFSETS = (0, -1, 1, 2)


def far_first():
    offs = [(a, b, c) for a in range(4) for b in range(4) for c in range(4) if a + b + c > 0]
    seen, groups = set(), []
    for o in offs:
        if o in seen:
            continue
        orbit = []
        for r in (o, (o[1], o[2], o[0]), (o[2], o[0], o[1])):
            for s in (r, tuple((-v) % 4 for v in r)):
                if s not in orbit:
                    orbit.append(s)
        seen.update(orbit)
        groups.append(orbit)
    groups.sort(key=lambda g: -sum(min(v, 4 - v) for v in g[0]))
    return [o for g in groups for o in g]


PEERS = far_first()


def sem_index(piece, phase, item, way):
    base = (0, 4, 20)[phase]
    return piece * 36 + base + item * 4 + way


def inverse_table():
    parts = []
    for dim in (64, 128):
        freqs = dim // 4
        inv = np.float32(theta) ** (-np.arange(freqs, dtype=np.float32) / np.float32(freqs))
        parts.append(np.broadcast_to(inv.astype(np.float32)[:, None], (freqs, 256)))
    return np.concatenate(parts, axis=0)


def rotate(x, cosr, sinr, cosc, sinc):
    f = x.shape[0] // 4
    a, b, c, d = x[:f], x[f : 2 * f], x[2 * f : 3 * f], x[3 * f :]
    return jnp.concatenate(
        [a * cosr - b * sinr, b * cosr + a * sinr, c * cosc - d * sinc, d * cosc + c * sinc], axis=0
    )


def normed_rows(x, gain):
    mean = jnp.mean(x * x, axis=0, keepdims=True)
    return x * lax.rsqrt(mean + eps) * gain


def gain_column(g_ref):
    g = g_ref[...]
    if g.shape[1] == 64:
        g = jnp.concatenate([g, g], axis=1)
    col = jnp.broadcast_to(g, (128, 128)).T
    return jnp.concatenate([col, col], axis=1)


def layer_kernel(
    qn_ref, kn_ref, vn_ref, qb_ref, kb_ref, vb_ref, gqn_ref, gkn_ref, gqb_ref, gkb_ref, inv_ref,
    stream_ref, ngain_ref, ids_ref, rw_ref, ow_hbm, gw_hbm, uw_hbm, dw_hbm,
    out_ref,
    kv, qna, qnb, qbt, s_scr, st_m, st_l, on, ob, heads, full, ow, gw, uw, dw, wide, normed,
    table, comb, sent, got, got2, part_a, part_b, part_c, ret, back,
    send_sem, recv_sem, tp_send, tp_recv, load_sem, d_send, d_recv, r_send, r_recv,
    f_send, f_recv, p_send, p_recv,
):
    sp = lax.axis_index("sp")
    tp = lax.axis_index("tp")
    me = (sp // 16, (sp // 4) % 4, sp % 4)

    def neighbour(dim, step):
        at = list(me)
        at[dim] = (at[dim] + step + 4) % 4
        return (at[0] * 4 + at[1]) * 4 + at[2]

    def chip_at(offset, sign):
        at = [(me[d] + sign * offset[d] + 4) % 4 for d in range(3)]
        return (at[0] * 4 + at[1]) * 4 + at[2]

    barrier = pltpu.get_barrier_semaphore()
    for o in PEERS:
        pl.semaphore_signal(barrier, inc=1, device_id=(chip_at(o, 1), tp), device_id_type=MESH)
    pl.semaphore_signal(barrier, inc=1, device_id=(sp, 1 - tp), device_id_type=MESH)

    loads = [
        pltpu.make_async_copy(ow_hbm, ow, load_sem.at[0]),
        pltpu.make_async_copy(gw_hbm.at[0], gw, load_sem.at[1]),
        pltpu.make_async_copy(uw_hbm.at[0], uw, load_sem.at[2]),
        pltpu.make_async_copy(dw_hbm.at[0], dw, load_sem.at[3]),
    ]
    for load in loads:
        load.start()

    lane = lax.broadcasted_iota(jnp.int32, (8, 256), 1)
    rows_of = ((lane // 128) + sp * 2).astype(F32)
    cols_of = (lane % 128).astype(F32)

    def tables(first, freqs):
        inv = inv_ref[first : first + freqs, :]
        r = jnp.concatenate([rows_of] * (freqs // 8), axis=0) * inv
        c = jnp.concatenate([cols_of] * (freqs // 8), axis=0) * inv
        return jnp.cos(r), jnp.sin(r), jnp.cos(c), jnp.sin(c)

    tab_n = tables(0, 16)
    tab_b = tables(16, 32)

    kt = rotate(normed_rows(kn_ref[...].astype(F32), gain_column(gkn_ref)[:64]), *tab_n)
    vt = vn_ref[...]
    here = kv.at[me[0], me[1], me[2]]
    here[0:128, :] = jnp.concatenate([kt[:, :128], kt[:, 128:]], axis=0).T.astype(BF)
    here[128:256, :] = jnp.concatenate([vt[:, :128], vt[:, 128:]], axis=0)
    kbt = rotate(normed_rows(kb_ref[...].astype(F32).T, gain_column(gkb_ref)), *tab_b)
    keys_b = kbt.T.astype(BF)
    vbt = vb_ref[...].astype(F32).T.astype(BF)
    here[256:512, :] = jnp.concatenate([keys_b[:128], vbt[:, :128]], axis=0)
    here[512:768, :] = jnp.concatenate([keys_b[128:], vbt[:, 128:]], axis=0)

    pl.semaphore_wait(barrier, 64)

    def part(piece, phase, item, way, mine):
        order = ORDERS[piece]
        at = [me[0], me[1], me[2]]
        rows = pl.ds(piece * 256, 256)
        if phase == 1:
            at[order[0]] = (me[order[0]] + OFFSETS[item] + 4) % 4
        if phase == 2:
            at[order[1]] = (me[order[1]] + OFFSETS[item] + 4) % 4
            at[order[0]] = pl.ds(0, 4)
        back = (0, 0, -1, 1)[way] if mine else (-1, 1, -2, 2)[way]
        if phase < 2 and mine:
            back = 0
        at[order[phase]] = (me[order[phase]] + back + 4) % 4
        if phase == 2 and way >= 2:
            at[order[0]] = pl.ds((way - 2) * 2, 2)
        return kv.at[at[0], at[1], at[2], rows]

    def copy_of(piece, phase, item, way, mine):
        ref = part(piece, phase, item, way, mine)
        index = sem_index(piece, phase, item, way)
        step = (1, -1, 1 if phase == 2 else 2, -1)[way]
        return pltpu.make_async_remote_copy(
            src_ref=ref, dst_ref=ref, send_sem=send_sem.at[index], recv_sem=recv_sem.at[index],
            device_id=(neighbour(ORDERS[piece][phase], step), tp), device_id_type=MESH,
        )

    def send(piece, phase, item, ways):
        for way in ways:
            copy_of(piece, phase, item, way, True).start()

    def arrive(piece, phase, item, way):
        copy_of(piece, phase, item, way, False).wait_recv()
        if phase == 2 and way < 2:
            copy_of(piece, phase, item, way + 2, True).start()

    pieces = range(3)
    for p in pieces:
        send(p, 0, 0, (0, 1, 2))
    for p in pieces:
        send(p, 1, 0, (0, 1, 2))

    zero = jnp.zeros((64, 256), BF)
    gq = gain_column(gqn_ref)[:64]
    for pair in range(4):
        qt = qn_ref[:, pair * 128 : pair * 128 + 128].astype(F32).T
        for half in range(2):
            h = pair * 2 + half
            q = rotate(normed_rows(qt[half * 64 : half * 64 + 64], gq), *tab_n).astype(BF)
            q = q.astype(F32) * (64 ** -0.5 * LOG2E)
            hi = q.astype(BF)
            lo = (q - hi.astype(F32)).astype(BF)
            qna[h] = jnp.concatenate([hi, zero, lo, zero], axis=0)
            qnb[h] = jnp.concatenate([zero, hi, zero, lo], axis=0)
    gq = gain_column(gqb_ref)
    for h in range(4):
        qt = qb_ref[:, h * 128 : h * 128 + 128].astype(F32).T
        q = rotate(normed_rows(qt, gq), *tab_b).astype(BF)
        q = q.astype(F32) * (128 ** -0.5 * LOG2E)
        hi = q.astype(BF)
        lo = (q - hi.astype(F32)).astype(BF)
        qbt[h] = jnp.concatenate([hi, lo], axis=0)

    slot = lax.broadcasted_iota(jnp.int32, (512, 128), 0)
    expert = slot // 8
    ids = ids_ref[...]
    first = expert == ids[0:1]
    second_ = expert == ids[1:2]
    hits = jnp.where(jnp.logical_or(first, second_), 1.0, 0.0)
    before = lax.broadcasted_iota(jnp.int32, (128, 128), 0) < lax.broadcasted_iota(jnp.int32, (128, 128), 1)
    ranks = jnp.dot(hits.astype(BF), jnp.where(before, 1.0, 0.0).astype(BF), preferred_element_type=F32)
    chosen = jnp.where(ranks == (slot % 8).astype(F32), hits, 0.0)
    table[...] = chosen.astype(BF)
    rw = rw_ref[...]
    weight = (chosen * (jnp.where(first, rw[0:1], 0.0) + jnp.where(second_, rw[1:2], 0.0))).T
    weight_hi = weight.astype(BF)
    comb[:, 0:512] = weight_hi
    comb[:, 512:1024] = (weight - weight_hi.astype(F32)).astype(BF)

    st_m[...] = jnp.full(st_m.shape, -1e30, F32)
    st_l[...] = jnp.zeros(st_l.shape, F32)
    on[...] = jnp.zeros(on.shape, F32)
    ob[...] = jnp.zeros(ob.shape, F32)

    def column_max(s):
        return jnp.max(s.reshape(-1, 8, 256), axis=0)

    def rows_at(piece, at, first, last):
        place = [slice(None), slice(None), slice(None)]
        place[ORDERS[piece][1]] = at[piece][0]
        place[ORDERS[piece][2]] = at[piece][1]
        blocks = kv[place[0], place[1], place[2], piece * 256 + first : piece * 256 + last, :]
        return [blocks[u] for u in range(4)]

    def qk(t, at, slot):
        mx = None
        for half in range(2):
            k = jnp.concatenate(rows_at(0 if t < 8 else 1 + half, at, 0, 128), axis=0)
            q = (qna, qnb)[half][t] if t < 8 else qbt[t - 8]
            s = jnp.dot(jnp.concatenate([k, k], axis=1), q, preferred_element_type=F32)
            s_scr[slot, pl.ds(half * 512, 512), :] = s
            r = column_max(s)
            mx = r if mx is None else jnp.maximum(mx, r)
        return mx

    def pv(t, at, slot, mx):
        m_old = st_m[t]
        mm = jnp.max(jnp.maximum(mx, m_old), axis=0, keepdims=True)
        alpha = jnp.exp2(m_old[0:1] - mm)
        ps, vs, ls = [], [], None
        for half in range(2):
            p = jnp.exp2(s_scr[slot, pl.ds(half * 512, 512), :] - mm)
            l = jnp.sum(p.reshape(-1, 8, 256), axis=0)
            ls = l if ls is None else ls + l
            ps.append(p.astype(BF))
            if t < 8:
                vs += rows_at(0, at, 128 + 64 * half, 192 + 64 * half)
            else:
                vs += rows_at(1 + half, at, 128, 256)
        o = jnp.dot(jnp.concatenate(vs, axis=1), jnp.concatenate(ps, axis=0), preferred_element_type=F32)
        st_m[t] = jnp.broadcast_to(mm, (8, 256))
        st_l[t] = st_l[t] * alpha + ls
        if t < 8:
            on[t] = on[t] * alpha + o
        else:
            ob[t - 8] = ob[t - 8] * alpha + o

    def opening():
        for way in range(3):
            for p in pieces:
                arrive(p, 0, 0, way)
                send(p, 1, way + 1, (0, 1))
        for p in pieces:
            for item in (1, 2, 3):
                send(p, 1, item, (2,))
        for p in pieces:
            send(p, 2, 0, (0, 1))

    def second():
        for way in range(2):
            for p in pieces:
                for item in range(4):
                    arrive(p, 1, item, way)
                send(p, 2, way + 1, (0, 1))

    def third():
        for p in pieces:
            for item in range(4):
                arrive(p, 1, item, 2)
            send(p, 2, 3, (0, 1))

    def sides(item):
        for p in pieces:
            arrive(p, 2, item, 0)
            arrive(p, 2, item, 1)

    def far(item):
        for p in pieces:
            arrive(p, 2, item, 2)
            arrive(p, 2, item, 3)

    events = {1: second, 3: third}
    for k in range(4):
        events[4 + 2 * k] = functools.partial(sides, k)
        events[12 + k] = functools.partial(far, k)

    def chunk_offset(c):
        return (c % 2) * 3 * (1 - c // 2) + (c // 2) * (1 + c % 2)

    def places(i):
        early = 1 - jnp.minimum(i // 4, 1)
        late = i // 12
        middle = 1 - early - late
        k = i - 4
        c = chunk_offset(early * i + middle * (k // 2) + late * (i - 12))
        side = middle * (3 - 2 * (k % 2)) + late * 2
        return [((me[o[1]] + c) % 4, (me[o[2]] + side) % 4) for o in ORDERS]

    def attend(i, mx):
        for at, event in events.items():
            pl.when(i == at)(event)
        now = places(i)
        nx = qk(0, now, 0)
        pv(11, places(jnp.maximum(i - 1, 0)), 1, mx)
        for t in range(11):
            mx = nx
            nx = qk(t + 1, now, (t + 1) % 2)
            pv(t, now, t % 2, mx)
        return nx

    opening()
    s_scr[1] = jnp.full((1024, 256), -1e30, F32)
    mx = lax.fori_loop(0, 16, attend, jnp.full((8, 256), -1e30, F32))
    pv(11, places(15), 1, mx)

    for pair in range(4):
        cols = []
        for t in (2 * pair, 2 * pair + 1):
            cols.append(on[t] / jnp.sum(st_l[t], axis=0, keepdims=True))
        heads[:, pair * 128 : pair * 128 + 128] = jnp.concatenate(cols, axis=0).T.astype(BF)
    for t in range(4):
        o = ob[t] / jnp.sum(st_l[8 + t], axis=0, keepdims=True)
        heads[:, 512 + t * 128 : 640 + t * 128] = o.T.astype(BF)

    mine = pl.ds(pl.multiple_of(tp * 128, 128), 128)
    other = pl.ds(pl.multiple_of((1 - tp) * 128, 128), 128)
    swaps = []
    for g in range(2):
        place = pl.ds(pl.multiple_of(g * 1024 + tp * 512, 128), 512)
        swap = pltpu.make_async_remote_copy(
            src_ref=heads.at[other, pl.ds(g * 512, 512)], dst_ref=full.at[:, place],
            send_sem=tp_send.at[g], recv_sem=tp_recv.at[g], device_id=(sp, 1 - tp), device_id_type=MESH,
        )
        swap.start()
        swaps.append(swap)
        full[:, place] = heads[mine, pl.ds(g * 512, 512)]
    for g in range(2):
        place = pl.ds(pl.multiple_of(g * 1024 + (1 - tp) * 512, 128), 512)
        pltpu.make_async_remote_copy(
            src_ref=heads.at[other, pl.ds(g * 512, 512)], dst_ref=full.at[:, place],
            send_sem=tp_send.at[g], recv_sem=tp_recv.at[g], device_id=(sp, 1 - tp), device_id_type=MESH,
        ).wait_recv()
        swaps[g].wait_send()

    for load in loads:
        load.wait()
    squares = jnp.zeros((128, 128), F32)
    for b in range(4):
        cols = slice(b * 512, b * 512 + 512)
        m = jnp.dot(full[...], ow[:, cols], preferred_element_type=F32)
        m = (stream_ref[:, cols].astype(F32) + m).astype(BF)
        wide[:, cols] = m
        m = m.astype(F32)
        m = m * m
        squares = squares + ((m[:, 0:128] + m[:, 128:256]) + (m[:, 256:384] + m[:, 384:512]))
    scale = lax.rsqrt(jnp.sum(squares, axis=1, keepdims=True) / 2048 + eps)
    for b in range(4):
        cols = slice(b * 512, b * 512 + 512)
        normed[:, cols] = (wide[:, cols].astype(F32) * scale * ngain_ref[:, cols]).astype(BF)

    for b in range(8):
        cols = slice(b * 256, b * 256 + 256)
        rows = jnp.dot(table[...], normed[:, cols], preferred_element_type=F32)
        sent[:, :, cols] = rows.reshape(64, 8, 256).astype(BF)

    def dispatch(n):
        to = chip_at(PEERS[n], 1)
        return pltpu.make_async_remote_copy(
            src_ref=sent.at[to], dst_ref=got.at[n], send_sem=d_send.at[n], recv_sem=d_recv.at[n],
            device_id=(to, tp), device_id_type=MESH,
        )

    def giveback(n):
        to = chip_at(PEERS[n], -1)
        return pltpu.make_async_remote_copy(
            src_ref=ret.at[n], dst_ref=back.at[sp], send_sem=r_send.at[n], recv_sem=r_recv.at[n],
            device_id=(to, tp), device_id_type=MESH,
        )

    def given(n):
        at = chip_at(PEERS[n], 1)
        return pltpu.make_async_remote_copy(
            src_ref=ret.at[n], dst_ref=back.at[at], send_sem=r_send.at[n], recv_sem=r_recv.at[n],
            device_id=(at, tp), device_id_type=MESH,
        )

    for n in range(63):
        dispatch(n).start()
    got[63] = sent[sp]

    def forward(c):
        rows = pl.ds(c * 16, 16)
        return pltpu.make_async_remote_copy(
            src_ref=got.at[rows], dst_ref=got2.at[rows], send_sem=f_send.at[c], recv_sem=f_recv.at[c],
            device_id=(sp, 1 - tp), device_id_type=MESH,
        )

    def partial(c):
        return pltpu.make_async_remote_copy(
            src_ref=part_b.at[c], dst_ref=part_c.at[c], send_sem=p_send.at[c], recv_sem=p_recv.at[c],
            device_id=(sp, 1 - tp), device_id_type=MESH,
        )

    for c in range(4):
        members = [n for n in range(c * 16, c * 16 + 16) if n < 63]
        for n in members:
            dispatch(n).wait_recv()
        forward(c).start()
        forward(c).wait_recv()
        rows = jnp.concatenate(
            [got[c * 16 : c * 16 + 16].reshape(128, 2048), got2[c * 16 : c * 16 + 16].reshape(128, 2048)], axis=0
        )
        gate = jnp.dot(rows, gw[...], preferred_element_type=F32)
        upper = jnp.dot(rows, uw[...], preferred_element_type=F32)
        hidden = (gate / (1.0 + jnp.exp(-gate)) * upper).astype(BF)
        for b in range(4):
            cols = slice(b * 512, b * 512 + 512)
            piece = jnp.dot(hidden, dw[:, cols], preferred_element_type=F32).astype(BF)
            part_a[:, cols] = piece[:128]
            part_b[c, :, cols] = piece[128:]
        partial(c).start()
        partial(c).wait_recv()
        total = (part_a[...].astype(F32) + part_c[c].astype(F32)).astype(BF)
        ret[c * 16 : c * 16 + 16] = total.reshape(16, 8, 2048)
        for n in members:
            giveback(n).start()
    back[sp] = ret[63]
    for n in range(63):
        given(n).wait_recv()
    rows = back[...].reshape(512, 2048)
    for b in range(4):
        cols = slice(b * 512, b * 512 + 512)
        piece = rows[:, cols]
        routed = jnp.dot(comb[...], jnp.concatenate([piece, piece], axis=0), preferred_element_type=F32)
        out_ref[:, cols] = (wide[:, cols].astype(F32) + routed).astype(BF)
    for n in range(63):
        dispatch(n).wait_send()
        giveback(n).wait_send()
    for c in range(4):
        forward(c).wait_send()
        partial(c).wait_send()
    for p in pieces:
        for phase in range(3):
            for item in range(1 if phase == 0 else 4):
                for way in range(4 if phase == 2 else 3):
                    copy_of(p, phase, item, way, True).wait_send()


def layer(
    stream, qn, kn, vn, qb, kb, vb, gqn, gkn, gqb, gkb, ow, ngain, gw, uw, dw, route_ids, route_weights
):
    inv = jnp.asarray(inverse_table())
    vm = pl.BlockSpec(memory_space=pltpu.VMEM)
    return pl.pallas_call(
        layer_kernel,
        out_shape=jax.ShapeDtypeStruct((128, 2048), BF),
        in_specs=[vm] * 15 + [pl.BlockSpec(memory_space=pl.ANY)] * 4,
        out_specs=vm,
        scratch_shapes=[
            pltpu.VMEM((4, 4, 4, 768, 128), BF),
            pltpu.VMEM((8, 256, 256), BF),
            pltpu.VMEM((8, 256, 256), BF),
            pltpu.VMEM((4, 256, 256), BF),
            pltpu.VMEM((2, 1024, 256), F32),
            pltpu.VMEM((12, 8, 256), F32),
            pltpu.VMEM((12, 8, 256), F32),
            pltpu.VMEM((8, 64, 256), F32),
            pltpu.VMEM((4, 128, 256), F32),
            pltpu.VMEM((256, 1024), BF),
            pltpu.VMEM((128, 2048), BF),
            pltpu.VMEM((2048, 2048), BF),
            pltpu.VMEM((2048, 512), BF),
            pltpu.VMEM((2048, 512), BF),
            pltpu.VMEM((512, 2048), BF),
            pltpu.VMEM((128, 2048), BF),
            pltpu.VMEM((128, 2048), BF),
            pltpu.VMEM((512, 128), BF),
            pltpu.VMEM((128, 1024), BF),
            pltpu.VMEM((64, 8, 2048), BF),
            pltpu.VMEM((64, 8, 2048), BF),
            pltpu.VMEM((64, 8, 2048), BF),
            pltpu.VMEM((128, 2048), BF),
            pltpu.VMEM((4, 128, 2048), BF),
            pltpu.VMEM((4, 128, 2048), BF),
            pltpu.VMEM((64, 8, 2048), BF),
            pltpu.VMEM((64, 8, 2048), BF),
            pltpu.SemaphoreType.DMA((108,)),
            pltpu.SemaphoreType.DMA((108,)),
            pltpu.SemaphoreType.DMA((2,)),
            pltpu.SemaphoreType.DMA((2,)),
            pltpu.SemaphoreType.DMA((4,)),
            pltpu.SemaphoreType.DMA((63,)),
            pltpu.SemaphoreType.DMA((63,)),
            pltpu.SemaphoreType.DMA((63,)),
            pltpu.SemaphoreType.DMA((63,)),
            pltpu.SemaphoreType.DMA((4,)),
            pltpu.SemaphoreType.DMA((4,)),
            pltpu.SemaphoreType.DMA((4,)),
            pltpu.SemaphoreType.DMA((4,)),
        ],
        compiler_params=pltpu.CompilerParams(
            collective_id=0, has_side_effects=True, vmem_limit_bytes=67043328
        ),
        name="layer",
    )(
        qn, kn.T, vn.T, qb, kb, vb,
        gqn.reshape(1, -1), gkn.reshape(1, -1), gqb.reshape(1, -1), gkb.reshape(1, -1), inv,
        stream, ngain.reshape(1, -1), route_ids.T, route_weights.T, ow, gw, uw, dw,
    )


def solution(mesh):
    return jax.shard_map(
        layer,
        mesh=mesh,
        in_specs=(
            P(("sp", "tp"), None),
            P("sp", "tp"),
            P("sp", "tp"),
            P("sp", "tp"),
            P("sp", "tp"),
            P("sp", "tp"),
            P("sp", "tp"),
            P(),
            P(),
            P(),
            P(),
            P(),
            P(),
            P("sp", None, "tp"),
            P("sp", None, "tp"),
            P("sp", "tp", None),
            P(("sp", "tp"), None),
            P(("sp", "tp"), None),
        ),
        out_specs=P(("sp", "tp"), None),
        check_vma=False,
    )
```

```python
import functools
import math

import jax
import jax.numpy as jnp
import numpy as np
from jax import lax
from jax.experimental import pallas as pl
from jax.experimental.pallas import tpu as pltpu
from jax.sharding import PartitionSpec as P

F32 = jnp.float32
BF = jnp.bfloat16
MESH = pl.DeviceIdType.MESH
eps = 1e-06
theta = 10000.0
LOG2E = math.log2(math.e)
ORDERS = ((2, 1, 0), (1, 0, 2), (0, 2, 1))
OFFSETS = (0, -1, 1, 2)


def far_first():
    offs = [(a, b, c) for a in range(4) for b in range(4) for c in range(4) if a + b + c > 0]
    seen, groups = set(), []
    for o in offs:
        if o in seen:
            continue
        orbit = []
        for r in (o, (o[1], o[2], o[0]), (o[2], o[0], o[1])):
            for s in (r, tuple((-v) % 4 for v in r)):
                if s not in orbit:
                    orbit.append(s)
        seen.update(orbit)
        groups.append(orbit)
    groups.sort(key=lambda g: -sum(min(v, 4 - v) for v in g[0]))
    return [o for g in groups for o in g]


PEERS = far_first()


def sem_index(piece, phase, item, way):
    base = (0, 4, 20)[phase]
    return piece * 36 + base + item * 4 + way


def inverse_table():
    parts = []
    for dim in (64, 128):
        freqs = dim // 4
        inv = np.float32(theta) ** (-np.arange(freqs, dtype=np.float32) / np.float32(freqs))
        parts.append(np.broadcast_to(inv.astype(np.float32)[:, None], (freqs, 256)))
    return np.concatenate(parts, axis=0)


def rotate(x, cosr, sinr, cosc, sinc):
    f = x.shape[0] // 4
    a, b, c, d = x[:f], x[f : 2 * f], x[2 * f : 3 * f], x[3 * f :]
    return jnp.concatenate(
        [a * cosr - b * sinr, b * cosr + a * sinr, c * cosc - d * sinc, d * cosc + c * sinc], axis=0
    )


def normed_rows(x, gain):
    mean = jnp.mean(x * x, axis=0, keepdims=True)
    return x * lax.rsqrt(mean + eps) * gain


def gain_column(g_ref):
    g = g_ref[...]
    if g.shape[1] == 64:
        g = jnp.concatenate([g, g], axis=1)
    col = jnp.broadcast_to(g, (128, 128)).T
    return jnp.concatenate([col, col], axis=1)


def layer_kernel(
    qn_ref, kn_ref, vn_ref, qb_ref, kb_ref, vb_ref, gqn_ref, gkn_ref, gqb_ref, gkb_ref, inv_ref,
    stream_ref, ngain_ref, ids_ref, rw_ref, ow_hbm, gw_hbm, uw_hbm, dw_hbm,
    out_ref,
    kv, qna, qnb, qbt, s_scr, st_m, st_l, on, ob, heads, full, ow, gw, uw, dw, wide, normed,
    table, comb, sent, got, got2, part_a, part_b, part_c, ret, back,
    send_sem, recv_sem, tp_send, tp_recv, load_sem, d_send, d_recv, r_send, r_recv,
    f_send, f_recv, p_send, p_recv,
):
    sp = lax.axis_index("sp")
    tp = lax.axis_index("tp")
    me = (sp // 16, (sp // 4) % 4, sp % 4)

    moved = [[(me[d] + step) % 4 for step in range(4)] for d in range(3)]

    def coordinate(dim, step):
        return moved[dim][step % 4]

    weights_of = (16, 4, 1)
    chips = [[sp + (moved[d][step] - me[d]) * weights_of[d] for step in range(4)] for d in range(3)]

    def neighbour(dim, step):
        return chips[dim][step % 4]

    def chip_at(offset, sign):
        at = [(me[d] + sign * offset[d] + 4) % 4 for d in range(3)]
        return (at[0] * 4 + at[1]) * 4 + at[2]

    barrier = pltpu.get_barrier_semaphore()
    for dim in range(3):
        for step in (1, 2, 3):
            pl.semaphore_signal(barrier, inc=1, device_id=(neighbour(dim, step), tp), device_id_type=MESH)
    pl.semaphore_signal(barrier, inc=1, device_id=(sp, 1 - tp), device_id_type=MESH)

    loads = [
        pltpu.make_async_copy(ow_hbm, ow, load_sem.at[0]),
        pltpu.make_async_copy(gw_hbm.at[0], gw, load_sem.at[1]),
        pltpu.make_async_copy(uw_hbm.at[0], uw, load_sem.at[2]),
        pltpu.make_async_copy(dw_hbm.at[0], dw, load_sem.at[3]),
    ]
    for load in loads:
        load.start()

    lane = lax.broadcasted_iota(jnp.int32, (8, 256), 1)
    rows_of = ((lane // 128) + sp * 2).astype(F32)
    cols_of = (lane % 128).astype(F32)

    def tables(first, freqs):
        inv = inv_ref[first : first + freqs, :]
        r = jnp.concatenate([rows_of] * (freqs // 8), axis=0) * inv
        c = jnp.concatenate([cols_of] * (freqs // 8), axis=0) * inv
        return jnp.cos(r), jnp.sin(r), jnp.cos(c), jnp.sin(c)

    tab_n = tables(0, 16)
    tab_b = tables(16, 32)

    kt = rotate(normed_rows(kn_ref[...].astype(F32), gain_column(gkn_ref)[:64]), *tab_n)
    vt = vn_ref[...]
    here = kv.at[me[0], me[1], me[2]]
    here[0:128, :] = jnp.concatenate([kt[:, :128], kt[:, 128:]], axis=0).T.astype(BF)
    here[128:256, :] = jnp.concatenate([vt[:, :128], vt[:, 128:]], axis=0)
    kbt = rotate(normed_rows(kb_ref[...].astype(F32).T, gain_column(gkb_ref)), *tab_b)
    keys_b = kbt.T.astype(BF)
    vbt = vb_ref[...].astype(F32).T.astype(BF)
    here[256:512, :] = jnp.concatenate([keys_b[:128], vbt[:, :128]], axis=0)
    here[512:768, :] = jnp.concatenate([keys_b[128:], vbt[:, 128:]], axis=0)

    pl.semaphore_wait(barrier, 10)

    def part(piece, phase, item, way, mine):
        order = ORDERS[piece]
        at = [me[0], me[1], me[2]]
        rows = pl.ds(piece * 256, 256)
        if phase == 1:
            at[order[0]] = coordinate(order[0], OFFSETS[item])
        if phase == 2:
            at[order[1]] = coordinate(order[1], OFFSETS[item])
            at[order[0]] = pl.ds(0, 4)
        back = (0, 0, -1, 1)[way] if mine else (-1, 1, -2, 2)[way]
        if phase < 2 and mine:
            back = 0
        at[order[phase]] = coordinate(order[phase], back)
        if phase == 2 and way >= 2:
            at[order[0]] = pl.ds((way - 2) * 2, 2)
        return kv.at[at[0], at[1], at[2], rows]

    def copy_of(piece, phase, item, way, mine):
        ref = part(piece, phase, item, way, mine)
        index = sem_index(piece, phase, item, way)
        step = (1, -1, 1 if phase == 2 else 2, -1)[way]
        return pltpu.make_async_remote_copy(
            src_ref=ref, dst_ref=ref, send_sem=send_sem.at[index], recv_sem=recv_sem.at[index],
            device_id=(neighbour(ORDERS[piece][phase], step), tp), device_id_type=MESH,
        )

    def send(piece, phase, item, ways):
        for way in ways:
            copy_of(piece, phase, item, way, True).start()

    def arrive(piece, phase, item, way):
        copy_of(piece, phase, item, way, False).wait_recv()
        if phase == 2 and way < 2:
            copy_of(piece, phase, item, way + 2, True).start()

    pieces = range(3)
    for p in pieces:
        send(p, 0, 0, (0, 1, 2))
    for p in pieces:
        send(p, 1, 0, (0, 1))

    zero = jnp.zeros((64, 256), BF)
    gq = gain_column(gqn_ref)[:64]
    for pair in range(4):
        qt = qn_ref[:, pair * 128 : pair * 128 + 128].astype(F32).T
        for half in range(2):
            h = pair * 2 + half
            q = rotate(normed_rows(qt[half * 64 : half * 64 + 64], gq), *tab_n).astype(BF)
            q = q.astype(F32) * (64 ** -0.5 * LOG2E)
            hi = q.astype(BF)
            lo = (q - hi.astype(F32)).astype(BF)
            qna[h] = jnp.concatenate([hi, zero, lo, zero], axis=0)
            qnb[h] = jnp.concatenate([zero, hi, zero, lo], axis=0)
    gq = gain_column(gqb_ref)
    for h in range(4):
        qt = qb_ref[:, h * 128 : h * 128 + 128].astype(F32).T
        q = rotate(normed_rows(qt, gq), *tab_b).astype(BF)
        q = q.astype(F32) * (128 ** -0.5 * LOG2E)
        hi = q.astype(BF)
        lo = (q - hi.astype(F32)).astype(BF)
        qbt[h] = jnp.concatenate([hi, lo], axis=0)

    slot = lax.broadcasted_iota(jnp.int32, (512, 128), 0)
    expert = slot // 8
    ids = ids_ref[...]
    first = expert == ids[0:1]
    second_ = expert == ids[1:2]
    hits = jnp.where(jnp.logical_or(first, second_), 1.0, 0.0)
    before = lax.broadcasted_iota(jnp.int32, (128, 128), 0) < lax.broadcasted_iota(jnp.int32, (128, 128), 1)
    ranks = jnp.dot(hits.astype(BF), jnp.where(before, 1.0, 0.0).astype(BF), preferred_element_type=F32)
    chosen = jnp.where(ranks == (slot % 8).astype(F32), hits, 0.0)
    table[...] = chosen.astype(BF)
    rw = rw_ref[...]
    weight = (chosen * (jnp.where(first, rw[0:1], 0.0) + jnp.where(second_, rw[1:2], 0.0))).T
    weight_hi = weight.astype(BF)
    comb[:, 0:512] = weight_hi
    comb[:, 512:1024] = (weight - weight_hi.astype(F32)).astype(BF)

    st_m[...] = jnp.full(st_m.shape, -1e30, F32)
    st_l[...] = jnp.zeros(st_l.shape, F32)
    on[...] = jnp.zeros(on.shape, F32)
    ob[...] = jnp.zeros(ob.shape, F32)

    def column_max(s):
        return jnp.max(s.reshape(-1, 8, 256), axis=0)

    def rows_at(piece, at, first, last):
        place = [slice(None), slice(None), slice(None)]
        place[ORDERS[piece][1]] = at[piece][0]
        place[ORDERS[piece][2]] = at[piece][1]
        blocks = kv[place[0], place[1], place[2], piece * 256 + first : piece * 256 + last, :]
        return [blocks[u] for u in range(4)]

    def qk(t, at, slot):
        mx = None
        for half in range(2):
            k = jnp.concatenate(rows_at(0 if t < 8 else 1 + half, at, 0, 128), axis=0)
            q = (qna, qnb)[half][t] if t < 8 else qbt[t - 8]
            s = jnp.dot(jnp.concatenate([k, k], axis=1), q, preferred_element_type=F32)
            s_scr[slot, pl.ds(half * 512, 512), :] = s
            r = column_max(s)
            mx = r if mx is None else jnp.maximum(mx, r)
        return mx

    def pv(t, at, slot, mx):
        m_old = st_m[t]
        mm = jnp.max(jnp.maximum(mx, m_old), axis=0, keepdims=True)
        alpha = jnp.exp2(m_old[0:1] - mm)
        ps, vs, ls = [], [], None
        for half in range(2):
            p = jnp.exp2(s_scr[slot, pl.ds(half * 512, 512), :] - mm)
            l = jnp.sum(p.reshape(-1, 8, 256), axis=0)
            ls = l if ls is None else ls + l
            ps.append(p.astype(BF))
            if t < 8:
                vs += rows_at(0, at, 128 + 64 * half, 192 + 64 * half)
            else:
                vs += rows_at(1 + half, at, 128, 256)
        o = jnp.dot(jnp.concatenate(vs, axis=1), jnp.concatenate(ps, axis=0), preferred_element_type=F32)
        st_m[t] = jnp.broadcast_to(mm, (8, 256))
        st_l[t] = st_l[t] * alpha + ls
        if t < 8:
            on[t] = on[t] * alpha + o
        else:
            ob[t - 8] = ob[t - 8] * alpha + o

    def opening():
        for way in range(3):
            for p in pieces:
                arrive(p, 0, 0, way)
                send(p, 1, way + 1, (0, 1))
        for p in pieces:
            for item in range(4):
                send(p, 1, item, (2,))
        for p in pieces:
            send(p, 2, 0, (0, 1))

    def second():
        for way in range(2):
            for p in pieces:
                for item in range(4):
                    arrive(p, 1, item, way)
                send(p, 2, way + 1, (0, 1))

    def third():
        for p in pieces:
            for item in range(4):
                arrive(p, 1, item, 2)
            send(p, 2, 3, (0, 1))

    def sides(item):
        for p in pieces:
            arrive(p, 2, item, 0)
            arrive(p, 2, item, 1)

    def far(item):
        for p in pieces:
            arrive(p, 2, item, 2)
            arrive(p, 2, item, 3)

    events = {1: second, 3: third}
    for k in range(4):
        events[4 + 2 * k] = functools.partial(sides, k)
        events[12 + k] = functools.partial(far, k)

    def chunk_offset(c):
        return (c % 2) * 3 * (1 - c // 2) + (c // 2) * (1 + c % 2)

    def places(i):
        early = 1 - jnp.minimum(i // 4, 1)
        late = i // 12
        middle = 1 - early - late
        k = i - 4
        c = chunk_offset(early * i + middle * (k // 2) + late * (i - 12))
        side = middle * (3 - 2 * (k % 2)) + late * 2
        return [((me[o[1]] + c) % 4, (me[o[2]] + side) % 4) for o in ORDERS]

    def attend(i, mx):
        for at, event in events.items():
            pl.when(i == at)(event)
        now = places(i)
        nx = qk(0, now, 0)
        pv(11, places(jnp.maximum(i - 1, 0)), 1, mx)
        for t in range(11):
            mx = nx
            nx = qk(t + 1, now, (t + 1) % 2)
            pv(t, now, t % 2, mx)
        return nx

    opening()
    s_scr[1] = jnp.full((1024, 256), -1e30, F32)
    mx = lax.fori_loop(0, 16, attend, jnp.full((8, 256), -1e30, F32))
    pv(11, places(15), 1, mx)

    for pair in range(4):
        cols = []
        for t in (2 * pair, 2 * pair + 1):
            cols.append(on[t] / jnp.sum(st_l[t], axis=0, keepdims=True))
        heads[:, pair * 128 : pair * 128 + 128] = jnp.concatenate(cols, axis=0).T.astype(BF)
    for t in range(4):
        o = ob[t] / jnp.sum(st_l[8 + t], axis=0, keepdims=True)
        heads[:, 512 + t * 128 : 640 + t * 128] = o.T.astype(BF)

    mine = pl.ds(pl.multiple_of(tp * 128, 128), 128)
    other = pl.ds(pl.multiple_of((1 - tp) * 128, 128), 128)
    swaps = []
    for g in range(2):
        place = pl.ds(pl.multiple_of(g * 1024 + tp * 512, 128), 512)
        swap = pltpu.make_async_remote_copy(
            src_ref=heads.at[other, pl.ds(g * 512, 512)], dst_ref=full.at[:, place],
            send_sem=tp_send.at[g], recv_sem=tp_recv.at[g], device_id=(sp, 1 - tp), device_id_type=MESH,
        )
        swap.start()
        swaps.append(swap)
        full[:, place] = heads[mine, pl.ds(g * 512, 512)]
    for g in range(2):
        place = pl.ds(pl.multiple_of(g * 1024 + (1 - tp) * 512, 128), 512)
        pltpu.make_async_remote_copy(
            src_ref=heads.at[other, pl.ds(g * 512, 512)], dst_ref=full.at[:, place],
            send_sem=tp_send.at[g], recv_sem=tp_recv.at[g], device_id=(sp, 1 - tp), device_id_type=MESH,
        ).wait_recv()
        swaps[g].wait_send()

    for load in loads:
        load.wait()
    squares = jnp.zeros((128, 128), F32)
    for b in range(4):
        cols = slice(b * 512, b * 512 + 512)
        m = jnp.dot(full[...], ow[:, cols], preferred_element_type=F32)
        m = (stream_ref[:, cols].astype(F32) + m).astype(BF)
        wide[:, cols] = m
        m = m.astype(F32)
        m = m * m
        squares = squares + ((m[:, 0:128] + m[:, 128:256]) + (m[:, 256:384] + m[:, 384:512]))
    scale = lax.rsqrt(jnp.sum(squares, axis=1, keepdims=True) / 2048 + eps)
    for b in range(4):
        cols = slice(b * 512, b * 512 + 512)
        normed[:, cols] = (wide[:, cols].astype(F32) * scale * ngain_ref[:, cols]).astype(BF)

    for b in range(8):
        cols = slice(b * 256, b * 256 + 256)
        rows = jnp.dot(table[...], normed[:, cols], preferred_element_type=F32)
        sent[:, :, cols] = rows.reshape(64, 8, 256).astype(BF)

    def dispatch(n):
        to = chip_at(PEERS[n], 1)
        return pltpu.make_async_remote_copy(
            src_ref=sent.at[to], dst_ref=got.at[n], send_sem=d_send.at[n], recv_sem=d_recv.at[n],
            device_id=(to, tp), device_id_type=MESH,
        )

    def giveback(n):
        to = chip_at(PEERS[n], -1)
        return pltpu.make_async_remote_copy(
            src_ref=ret.at[n], dst_ref=back.at[sp], send_sem=r_send.at[n], recv_sem=r_recv.at[n],
            device_id=(to, tp), device_id_type=MESH,
        )

    def given(n):
        at = chip_at(PEERS[n], 1)
        return pltpu.make_async_remote_copy(
            src_ref=ret.at[n], dst_ref=back.at[at], send_sem=r_send.at[n], recv_sem=r_recv.at[n],
            device_id=(at, tp), device_id_type=MESH,
        )

    for n in range(63):
        dispatch(n).start()
    got[63] = sent[sp]

    def forward(c):
        rows = pl.ds(c * 16, 16)
        return pltpu.make_async_remote_copy(
            src_ref=got.at[rows], dst_ref=got2.at[rows], send_sem=f_send.at[c], recv_sem=f_recv.at[c],
            device_id=(sp, 1 - tp), device_id_type=MESH,
        )

    def partial(c):
        return pltpu.make_async_remote_copy(
            src_ref=part_b.at[c], dst_ref=part_c.at[c], send_sem=p_send.at[c], recv_sem=p_recv.at[c],
            device_id=(sp, 1 - tp), device_id_type=MESH,
        )

    for c in range(4):
        members = [n for n in range(c * 16, c * 16 + 16) if n < 63]
        for n in members:
            dispatch(n).wait_recv()
        forward(c).start()
        forward(c).wait_recv()
        rows = jnp.concatenate(
            [got[c * 16 : c * 16 + 16].reshape(128, 2048), got2[c * 16 : c * 16 + 16].reshape(128, 2048)], axis=0
        )
        gate = jnp.dot(rows, gw[...], preferred_element_type=F32)
        upper = jnp.dot(rows, uw[...], preferred_element_type=F32)
        hidden = (gate / (1.0 + jnp.exp(-gate)) * upper).astype(BF)
        for b in range(4):
            cols = slice(b * 512, b * 512 + 512)
            piece = jnp.dot(hidden, dw[:, cols], preferred_element_type=F32).astype(BF)
            part_a[:, cols] = piece[:128]
            part_b[c, :, cols] = piece[128:]
        partial(c).start()
        partial(c).wait_recv()
        total = (part_a[...].astype(F32) + part_c[c].astype(F32)).astype(BF)
        ret[c * 16 : c * 16 + 16] = total.reshape(16, 8, 2048)
        for n in members:
            giveback(n).start()
    back[sp] = ret[63]
    for n in range(63):
        given(n).wait_recv()
    rows = back[...].reshape(512, 2048)
    for b in range(4):
        cols = slice(b * 512, b * 512 + 512)
        piece = rows[:, cols]
        routed = jnp.dot(comb[...], jnp.concatenate([piece, piece], axis=0), preferred_element_type=F32)
        out_ref[:, cols] = (wide[:, cols].astype(F32) + routed).astype(BF)
    for n in range(63):
        dispatch(n).wait_send()
        giveback(n).wait_send()
    for c in range(4):
        forward(c).wait_send()
        partial(c).wait_send()
    for p in pieces:
        for phase in range(3):
            for item in range(1 if phase == 0 else 4):
                for way in range(4 if phase == 2 else 3):
                    copy_of(p, phase, item, way, True).wait_send()


def layer(
    stream, qn, kn, vn, qb, kb, vb, gqn, gkn, gqb, gkb, ow, ngain, gw, uw, dw, route_ids, route_weights
):
    inv = jnp.asarray(inverse_table())
    vm = pl.BlockSpec(memory_space=pltpu.VMEM)
    return pl.pallas_call(
        layer_kernel,
        out_shape=jax.ShapeDtypeStruct((128, 2048), BF),
        in_specs=[vm] * 15 + [pl.BlockSpec(memory_space=pl.ANY)] * 4,
        out_specs=vm,
        scratch_shapes=[
            pltpu.VMEM((4, 4, 4, 768, 128), BF),
            pltpu.VMEM((8, 256, 256), BF),
            pltpu.VMEM((8, 256, 256), BF),
            pltpu.VMEM((4, 256, 256), BF),
            pltpu.VMEM((2, 1024, 256), F32),
            pltpu.VMEM((12, 8, 256), F32),
            pltpu.VMEM((12, 8, 256), F32),
            pltpu.VMEM((8, 64, 256), F32),
            pltpu.VMEM((4, 128, 256), F32),
            pltpu.VMEM((256, 1024), BF),
            pltpu.VMEM((128, 2048), BF),
            pltpu.VMEM((2048, 2048), BF),
            pltpu.VMEM((2048, 512), BF),
            pltpu.VMEM((2048, 512), BF),
            pltpu.VMEM((512, 2048), BF),
            pltpu.VMEM((128, 2048), BF),
            pltpu.VMEM((128, 2048), BF),
            pltpu.VMEM((512, 128), BF),
            pltpu.VMEM((128, 1024), BF),
            pltpu.VMEM((64, 8, 2048), BF),
            pltpu.VMEM((64, 8, 2048), BF),
            pltpu.VMEM((64, 8, 2048), BF),
            pltpu.VMEM((128, 2048), BF),
            pltpu.VMEM((4, 128, 2048), BF),
            pltpu.VMEM((4, 128, 2048), BF),
            pltpu.VMEM((64, 8, 2048), BF),
            pltpu.VMEM((64, 8, 2048), BF),
            pltpu.SemaphoreType.DMA((108,)),
            pltpu.SemaphoreType.DMA((108,)),
            pltpu.SemaphoreType.DMA((2,)),
            pltpu.SemaphoreType.DMA((2,)),
            pltpu.SemaphoreType.DMA((4,)),
            pltpu.SemaphoreType.DMA((63,)),
            pltpu.SemaphoreType.DMA((63,)),
            pltpu.SemaphoreType.DMA((63,)),
            pltpu.SemaphoreType.DMA((63,)),
            pltpu.SemaphoreType.DMA((4,)),
            pltpu.SemaphoreType.DMA((4,)),
            pltpu.SemaphoreType.DMA((4,)),
            pltpu.SemaphoreType.DMA((4,)),
        ],
        compiler_params=pltpu.CompilerParams(
            collective_id=0, has_side_effects=True, vmem_limit_bytes=67043328
        ),
        name="layer",
    )(
        qn, kn.T, vn.T, qb, kb, vb,
        gqn.reshape(1, -1), gkn.reshape(1, -1), gqb.reshape(1, -1), gkb.reshape(1, -1), inv,
        stream, ngain.reshape(1, -1), route_ids.T, route_weights.T, ow, gw, uw, dw,
    )


def solution(mesh):
    return jax.shard_map(
        layer,
        mesh=mesh,
        in_specs=(
            P(("sp", "tp"), None),
            P("sp", "tp"),
            P("sp", "tp"),
            P("sp", "tp"),
            P("sp", "tp"),
            P("sp", "tp"),
            P("sp", "tp"),
            P(),
            P(),
            P(),
            P(),
            P(),
            P(),
            P("sp", None, "tp"),
            P("sp", None, "tp"),
            P("sp", "tp", None),
            P(("sp", "tp"), None),
            P(("sp", "tp"), None),
        ),
        out_specs=P(("sp", "tp"), None),
        check_vma=False,
    )
```
